32 devices in a mesh: ep: 16 (over z, y, x), tp: 2 (over core).
Axes of the slice: x: 2, y: 2, z: 4, core: 2. Of those that a mesh axis runs over, the one named last changes fastest.
Arguments:
- tokens: bfloat16 [512, 3072], P('ep'), may hold values from -6 to 6
- carried: float32 [512, 96, 128], P('ep', 'tp'), may hold values from -4 to 4
- decay_rate: float32 [96, 64], P('tp'), may hold values from 0.02 to 20
- frequency: float32 [96, 64], P('tp'), may hold values from 0 to 200
- log_step: float32 [96], P('tp'), may hold values from -4.6 to 0
- in_map: bfloat16 [96, 128, 16], P('tp'), may hold values from -1 to 1
- out_map: bfloat16 [96, 16, 128], P('tp'), may hold values from -0.5 to 0.5
- skip_gain: float32 [1536], P('tp'), may hold values from -4 to 4
- norm_gain: float32 [3072], replicated, may hold values from 0.1 to 1.9
- w_in: bfloat16 [3072, 1536], P(None, 'tp'), may hold values from -0.109375 to 0.109375
- w_out: bfloat16 [1536, 3072], P('tp'), may hold values from -0.15625 to 0.15625
- expert_gain: float32 [3072], replicated, may hold values from 0.1 to 1.9
- route_ids: int32 [512, 2], P('ep'), may hold values from 0 to 7, all different within a row; in each aligned block of 32 rows (0 to 31, 32 to 63, ...) at most 16 rows name the same one
- route_logit: float32 [512, 2], P('ep'), may hold values from -6 to 6
- w_gate: bfloat16 [3072, 43008], P(None, ('ep', 'tp')), may hold values from -0.109375 to 0.109375
- w_up: bfloat16 [3072, 43008], P(None, ('ep', 'tp')), may hold values from -0.109375 to 0.109375
- w_down: bfloat16 [43008, 3072], P(('ep', 'tp')), may hold values from -0.078125 to 0.078125
Outputs:
- new_tokens: bfloat16 [512, 3072], P('ep', 'tp')
- new_carried: float32 [512, 96, 128], P('ep', 'tp')
The draws below stay inside these ranges and needn't reach their ends.
Inputs may be any that keep to these rules, and one draw needn't show every extreme that they name: `route_ids`: each row names 2 different experts; within each aligned block of 32 rows (the rows of one index of ep) no expert is named by more than 16 rows, a bound that some block reaches.
All inputs are finite; a program needn't handle non-finite values.
Results may differ from the reference program's by a relative error of at most 0.014.
Values may be sent and summed in bfloat16 or wider, within the bound.
A program may use at most 128 MiB of HBM per device.

```python
import math
import jax
import jax.numpy as jnp
import numpy as np
from jax import lax

D = 3072
GROUPS = 96
CH = 16
STATE = 64
FF = 5376
EXPERTS = 8
TOP = 2
SEQ_DEV = 32
SEQS = 512
WIDTH = 1536
CAP = 16
N_TP = 2


def block_scale(rng, dims, split, low, largest):
    loudness, own = 1.0, jax.random.fold_in(rng, 6)
    for dim, shards_of in split:
        steps = jnp.exp(jax.random.uniform(jax.random.fold_in(own, dim), (shards_of,), jnp.float32, low / len(split), largest / len(split)))
        loudness = loudness * jnp.repeat(steps, dims[dim] // shards_of).reshape([-1 if axis == dim else 1 for axis in range(len(dims))])
    return loudness


def shared_out(key, own, number, rows, amount, top, most, slope):
    ranking = jax.random.permutation(key, amount)
    heavy_load, usual = load_shares(amount, rows * top, most, slope, True), load_shares(amount, rows * top, most, slope, False)
    places = jnp.arange(amount)

    def named(sizes, turn):
        used = int((sizes > 0).sum())
        fixed = max(1, used // 4)
        moved = fixed + (places - fixed + turn * (used - fixed)) % max(1, amount - fixed)
        return jnp.zeros((amount,), jnp.int32).at[ranking[jnp.where(places < fixed, places, moved)]].set(jnp.asarray(sizes, jnp.int32))

    sizes = jnp.where(number % 4 == 0, named(heavy_load, number // 4), named(usual, number - number // 4 - 1))
    mixed = jax.random.permutation(jax.random.fold_in(own, 3), amount)
    giver, sink = mixed[0:amount // 2 * 2:2], mixed[1:amount // 2 * 2:2]
    slack = jnp.minimum(sizes[giver] - 1, most - sizes[sink]) // 2
    slack = jnp.where((giver == ranking[0]) | (sink == ranking[0]) | (sizes[sink] == 0), 0, jnp.maximum(slack, 0))
    moved = jax.random.randint(jax.random.fold_in(own, 4), (amount // 2,), 0, 1 << 20) % (slack + 1)
    sizes = sizes.at[giver].add(-moved).at[sink].add(moved)
    members = jnp.searchsorted(jnp.cumsum(sizes), jnp.arange(rows * top), side="right").astype(jnp.int32)
    grid = members.reshape(top, rows).T
    grid = grid[jax.random.permutation(jax.random.fold_in(own, 1), rows)]
    turn = jax.random.randint(jax.random.fold_in(own, 2), (rows, 1), 0, top)
    return jnp.take_along_axis(grid, (jnp.arange(top)[None, :] + turn) % top, axis=1)


def load_shares(amount, total, limit, slope, full):
    loads = [(1 << 20) // math.isqrt(standing ** slope) + 1 for standing in range(1, amount + 1)]
    largest = limit if full else min(limit, max(-(-total // amount), total * loads[0] // sum(loads)))
    least = 1 if total - largest >= amount - 1 else 0
    holding, rest = [largest] + [least] * (amount - 1), total - largest - least * (amount - 1)
    while rest > 0:
        movable = [i for i in range(1, amount) if holding[i] < largest] or [i for i in range(1, amount) if holding[i] < limit]
        whole, budget = sum([loads[i] for i in movable]), rest
        for i in movable:
            extra = min(limit - holding[i], max(1, budget * loads[i] // whole), rest)
            holding[i] = holding[i] + extra
            rest = rest - extra
    return np.array(holding)


def gaussian(stream_key, dims, scale, bound, cuts=(), dtype=jnp.bfloat16):
    level = block_scale(stream_key, dims, cuts, -0.22, 0.18) if cuts else 1.0
    array = jax.random.normal(stream_key, dims, jnp.float32) * scale * level
    return jnp.minimum(jnp.maximum(array, -bound), bound).astype(dtype)


def setup_inputs(seed: int = 0) -> dict:
    arg_keys = jax.random.split(jax.random.key(seed), 18)
    tokens = gaussian(arg_keys[0], (SEQS, D), 1.0, 6.0, ((0, 16),))
    carried = gaussian(arg_keys[1], (SEQS, GROUPS, 2 * STATE), 0.5, 4.0, ((0, 16), (1, 2)), jnp.float32)
    decay_rate = jnp.clip(jnp.exp(math.log(20.0) - 6.9077553 * jax.random.uniform(arg_keys[2], (GROUPS, STATE), jnp.float32) ** block_scale(arg_keys[2], (GROUPS, STATE), ((0, 2),), -0.2, 0.2)), 0.02, 20.0)
    frequency = jnp.clip(200.0 * jax.random.uniform(arg_keys[3], (GROUPS, STATE), jnp.float32) ** block_scale(arg_keys[3], (GROUPS, STATE), ((0, 2),), -0.2, 0.2), 0.0, 200.0)
    log_step = jnp.clip(-4.6 + 4.6 * jax.random.uniform(arg_keys[4], (GROUPS,), jnp.float32) ** block_scale(arg_keys[4], (GROUPS,), ((0, 2),), -0.2, 0.2), -4.6, 0.0)
    in_map = gaussian(arg_keys[5], (GROUPS, 2 * STATE, CH), (2 * CH) ** -0.5, 1.0, ((0, 2),))
    out_map = gaussian(arg_keys[6], (GROUPS, CH, 2 * STATE), (2 * STATE) ** -0.5, 0.5, ((0, 2),))
    skip_gain = gaussian(arg_keys[7], (WIDTH,), 1.0, 4.0, ((0, 2),), jnp.float32)
    norm_gain = jnp.clip(1.0 + 0.18 * jax.random.normal(arg_keys[8], (D,), jnp.float32), 0.1, 1.9)
    w_in = gaussian(arg_keys[9], (D, WIDTH), D ** -0.5, 0.109375, ((1, 2),))
    w_out = gaussian(arg_keys[10], (WIDTH, D), WIDTH ** -0.5, 0.15625, ((0, 2),))
    expert_gain = jnp.clip(1.0 + 0.18 * jax.random.normal(arg_keys[11], (D,), jnp.float32), 0.1, 1.9)
    route_ids_keys = jax.random.split(jax.random.fold_in(arg_keys[12], 1), SEQS // SEQ_DEV)
    route_ids_turns = jax.random.permutation(jax.random.fold_in(arg_keys[12], 3), SEQS // SEQ_DEV)
    route_ids = jax.vmap(lambda own, number: shared_out(jax.random.fold_in(arg_keys[12], 2), own, number, SEQ_DEV, EXPERTS, TOP, CAP, 1))(route_ids_keys, route_ids_turns).reshape((SEQS, TOP))
    route_logit = gaussian(arg_keys[13], (SEQS, TOP), 1.5, 6.0, ((0, 16),), jnp.float32)
    w_gate = gaussian(arg_keys[14], (D, EXPERTS * FF), D ** -0.5, 0.109375, ((1, 32),))
    w_up = gaussian(arg_keys[15], (D, EXPERTS * FF), D ** -0.5, 0.109375, ((1, 32),))
    w_down = gaussian(arg_keys[16], (EXPERTS * FF, D), FF ** -0.5, 0.078125, ((0, 32),))
    return dict(tokens=tokens, carried=carried, decay_rate=decay_rate, frequency=frequency, log_step=log_step, in_map=in_map, out_map=out_map, skip_gain=skip_gain, norm_gain=norm_gain, w_in=w_in, w_out=w_out, expert_gain=expert_gain, route_ids=route_ids, route_logit=route_logit, w_gate=w_gate, w_up=w_up, w_down=w_down)


def normalize(rows, gain):
    wide = rows.astype(jnp.float32)
    scaled = wide * lax.rsqrt(lax.optimization_barrier(jnp.mean(wide * wide, axis=-1, keepdims=True)) + 1e-06)
    return (scaled * gain).astype(jnp.bfloat16)

def state_update(drive, carried, decay_rate, frequency, log_step, in_map, out_map, skip_gain):
    count_rows, width = drive.shape
    groups, half = decay_rate.shape
    channels = width // groups
    step_size = jnp.exp(log_step)[:, None]
    magnitude = jnp.exp(-decay_rate * step_size)
    real_decay = magnitude * jnp.cos(frequency * step_size)
    imag_decay = magnitude * jnp.sin(frequency * step_size)
    denom = decay_rate * decay_rate + frequency * frequency
    real_less = real_decay - 1.0
    real_factor = (-real_less * decay_rate + imag_decay * frequency) / denom
    imag_factor = (-imag_decay * decay_rate - real_less * frequency) / denom
    wide_drive = drive.astype(jnp.float32).reshape(count_rows, groups, channels)
    projected = jnp.einsum('sgh,gqh->sgq', wide_drive, in_map.astype(jnp.float32))
    real_in = projected[..., :half]
    imag_in = projected[..., half:]
    real_push = real_factor * real_in - imag_factor * imag_in
    imag_push = real_factor * imag_in + imag_factor * real_in
    real_old = carried[..., :half]
    imag_old = carried[..., half:]
    real_new = real_decay * real_old - imag_decay * imag_old + real_push
    imag_new = real_decay * imag_old + imag_decay * real_old + imag_push
    joined = jnp.concatenate([real_new, -imag_new], axis=-1)
    reading = jnp.einsum('sgq,ghq->sgh', joined, out_map.astype(jnp.float32), precision=lax.Precision.HIGHEST)
    total = reading.reshape(count_rows, width) + skip_gain * drive.astype(jnp.float32)
    activated = jax.nn.gelu(total).astype(jnp.bfloat16)
    return (activated, jnp.concatenate([real_new, imag_new], axis=-1))

def route_weights(route_logit):
    first = jax.nn.sigmoid(route_logit[:, 0] - route_logit[:, 1])
    second = jax.nn.sigmoid(route_logit[:, 1] - route_logit[:, 0])
    return jnp.stack([first, second], axis=1)

def expert_output(rows, gate_cols, up_cols, down_rows):
    gated = jnp.dot(rows, gate_cols, preferred_element_type=jnp.float32)
    upward = jnp.dot(rows, up_cols, preferred_element_type=jnp.float32)
    hidden = (jax.nn.silu(gated) * upward).astype(jnp.bfloat16)
    return jnp.dot(hidden, down_rows, preferred_element_type=jnp.float32)

def reference(tokens, carried, decay_rate, frequency, log_step, in_map, out_map, skip_gain, norm_gain, w_in, w_out, expert_gain, route_ids, route_logit, w_gate, w_up, w_down):
    normed = normalize(tokens, norm_gain)
    drive = jnp.dot(normed, w_in, preferred_element_type=jnp.float32).astype(jnp.bfloat16)
    activated, new_carried = state_update(drive, carried, decay_rate, frequency, log_step, in_map, out_map, skip_gain)
    block = activated.shape[1] // N_TP
    summed = jnp.zeros(tokens.shape, jnp.float32)
    for index in range(N_TP):
        partial_value = jnp.dot(activated[:, index * block:(index + 1) * block], w_out[index * block:(index + 1) * block], preferred_element_type=jnp.float32).astype(jnp.bfloat16)
        summed = summed + partial_value.astype(jnp.float32)
    mixed = (tokens.astype(jnp.float32) + summed).astype(jnp.bfloat16)
    expert_in = normalize(mixed, expert_gain)
    weights = route_weights(route_logit)
    hidden_units = w_gate.shape[1] // EXPERTS
    total = mixed.astype(jnp.float32)
    for expert in range(EXPERTS):
        chosen = lax.optimization_barrier(jnp.sum(jnp.where(route_ids == expert, weights, 0.0), axis=1))
        lower = expert * hidden_units
        upper = lower + hidden_units
        produced = expert_output(expert_in, w_gate[:, lower:upper], w_up[:, lower:upper], w_down[lower:upper])
        total = total + chosen[:, None] * produced
    return (total.astype(jnp.bfloat16), new_carried)
```

```python
import functools

import jax
import jax.numpy as jnp
from jax import lax
from jax.experimental import pallas as pl
from jax.experimental.pallas import tpu as pltpu
from jax.sharding import PartitionSpec as P

EXPERTS = 8
TOP = 2
CAP = 16

MESH = pl.DeviceIdType.MESH
SEND_ORDER = (1, 2, 4, 6, 5, 7, 3)
WAIT_ORDER = (0, 1, 2, 4, 6, 5, 7, 3)
BACK_ORDER = (4, 6, 5, 7, 2, 3, 1)
CHUNKS = 3
PIECES = 6
LANES = 128
OUT_PARTS = 4
WEIGHT_PARTS = 3


def normalize(rows, gain):
    wide = rows.astype(jnp.float32)
    scaled = wide * lax.rsqrt(jnp.mean(wide * wide, axis=-1, keepdims=True) + 1e-06)
    return (scaled * gain).astype(jnp.bfloat16)


def dot_wide(left, right):
    return jnp.dot(left, right, preferred_element_type=jnp.float32)


def dot_transposed(left, right):
    return lax.dot_general(
        left, right, (((1,), (1,)), ((), ())), preferred_element_type=jnp.float32
    )


def gelu(value):
    inner = 0.7978845608028654 * (value + 0.044715 * (value * value * value))
    return value * (0.5 * (1.0 + jnp.tanh(inner)))


def coefficients(log_step, decay_rate, frequency, tables):
    groups, half = decay_rate.shape
    row = lax.broadcasted_iota(jnp.int32, (groups, groups), 0)
    column = lax.broadcasted_iota(jnp.int32, (groups, groups), 1)
    spread = jnp.where(row == column, jnp.broadcast_to(log_step, (groups, groups)), 0.0)
    step_size = jnp.exp(jnp.sum(spread, axis=1, keepdims=True))
    magnitude = jnp.exp(-decay_rate * step_size)
    real_decay = magnitude * jnp.cos(frequency * step_size)
    imag_decay = magnitude * jnp.sin(frequency * step_size)
    denom = decay_rate * decay_rate + frequency * frequency
    real_less = real_decay - 1.0
    real_factor = (-real_less * decay_rate + imag_decay * frequency) / denom
    imag_factor = (-imag_decay * decay_rate - real_less * frequency) / denom
    tables[0] = jnp.concatenate([real_decay, real_decay], axis=1)
    tables[1] = jnp.concatenate([imag_decay, -imag_decay], axis=1)
    tables[2] = jnp.concatenate([real_factor, real_factor], axis=1)
    tables[3] = jnp.concatenate([imag_factor, -imag_factor], axis=1)


def routing(ids, logit):
    count_rows = ids.shape[1]
    expert = lax.broadcasted_iota(jnp.int32, (EXPERTS, count_rows), 0)
    first = (ids[0:1, :] == expert).astype(jnp.float32)
    second = (ids[1:2, :] == expert).astype(jnp.float32)
    named = first + second
    weight = first * jax.nn.sigmoid(logit[0:1, :] - logit[1:2, :])
    weight = weight + second * jax.nn.sigmoid(logit[1:2, :] - logit[0:1, :])
    row = lax.broadcasted_iota(jnp.int32, (count_rows, count_rows), 0)
    column = lax.broadcasted_iota(jnp.int32, (count_rows, count_rows), 1)
    earlier = dot_wide(named, (row < column).astype(jnp.float32))
    slots = (EXPERTS, CAP, count_rows)
    slot = lax.broadcasted_iota(jnp.int32, slots, 1).astype(jnp.float32)
    here = slot == jnp.broadcast_to(earlier[:, None, :], slots)
    pack = jnp.where(here, jnp.broadcast_to(named[:, None, :], slots), 0.0)
    weighed = jnp.where(here, jnp.broadcast_to(weight[:, None, :], slots), 0.0)
    total = EXPERTS * CAP
    return pack.reshape(total, count_rows), weighed.reshape(total, count_rows)


def layer_kernel(
    group_size,
    tokens_hbm,
    carried_hbm,
    decay_hbm,
    frequency_hbm,
    log_step_hbm,
    in_map_hbm,
    out_map_hbm,
    skip_hbm,
    norm_gain_hbm,
    w_in_hbm,
    w_out_hbm,
    expert_gain_hbm,
    ids_hbm,
    logit_hbm,
    gate_hbm,
    up_hbm,
    down_hbm,
    out,
    new_carried,
    tokens,
    carried,
    decay_rate,
    frequency,
    log_step,
    in_map,
    out_map,
    skip,
    norm_gain,
    expert_gain,
    ids,
    logit,
    gate_up,
    dense,
    tables,
    spread_in,
    spread_out,
    joined,
    activated,
    partial,
    partial_in,
    mixed_buf,
    normed_buf,
    packed,
    rows_buf,
    gate_sum,
    up_sum,
    hidden_t,
    hidden,
    swap_out,
    swap_in,
    own_sum,
    peer_out,
    peer_in,
    back_out,
    returned,
    load_sem,
    weight_sem,
    partial_send,
    partial_recv,
    direct_recv,
    peer_recv,
    core_recv,
    swap_recv,
    sum_recv,
    back_recv,
    send_sem,
):
    ep = lax.axis_index("ep")
    core = lax.axis_index("tp")
    expert = ep // group_size
    lane = ep % group_size
    other = 1 - core
    count_rows, model_width = tokens.shape
    groups, states = decay_rate.shape
    width = skip.shape[0]
    channels = width // groups
    per_block = LANES // channels
    blocks = groups // per_block
    half = model_width // 2
    hidden_units = gate_hbm.shape[0]
    total_rows = group_size * EXPERTS * CAP
    in_parts = model_width // width
    gate, up = gate_up.at[0], gate_up.at[1]
    mix = dense.at[width : 2 * width]
    down = dense.at[:hidden_units]
    piece = half // PIECES
    chunk = half // CHUNKS

    def at_expert(step):
        place, bit = 0, 1
        while bit < EXPERTS:
            place = place + bit * lax.rem(expert // bit + step // bit, 2)
            bit *= 2
        return place

    def at_lane(step):
        return lax.rem(lane + step + group_size, group_size)

    loads = {}

    def load(name, source, target):
        loads[name] = pltpu.make_async_copy(source, target, load_sem.at[len(loads)])
        loads[name].start()

    load("tokens", tokens_hbm, tokens)
    load("norm_gain", norm_gain_hbm, norm_gain)
    for part in range(in_parts):
        span = pl.ds(part * width, width)
        load(("w_in", part), w_in_hbm.at[span], dense.at[:width, span])
    load("log_step", log_step_hbm, log_step)
    load("decay", decay_hbm, decay_rate)
    load("frequency", frequency_hbm, frequency)
    load("in_map", in_map_hbm, in_map)
    load("out_map", out_map_hbm, out_map)
    load("carried", carried_hbm, carried)
    load("skip", skip_hbm, skip)
    load("ids", ids_hbm, ids)
    load("logit", logit_hbm, logit)
    load("expert_gain", expert_gain_hbm, expert_gain)
    out_span = model_width // OUT_PARTS
    for part in range(OUT_PARTS):
        span = pl.ds(part * out_span, out_span)
        load(("w_out", part), w_out_hbm.at[:, span], mix.at[:, span])

    barrier = pltpu.get_barrier_semaphore()
    pl.semaphore_signal(barrier, inc=1, device_id=(ep, other), device_id_type=MESH)
    for step in range(1, EXPERTS):
        target = at_expert(step) * group_size + lane
        pl.semaphore_signal(barrier, inc=1, device_id=(target, core), device_id_type=MESH)
    for step in range(1, group_size):
        target = expert * group_size + at_lane(step)
        pl.semaphore_signal(barrier, inc=1, device_id=(target, core), device_id_type=MESH)

    weight_span = hidden_units // WEIGHT_PARTS

    def weight_copies(source, target, sem):
        for part in range(WEIGHT_PARTS):
            span = pl.ds(part * weight_span, weight_span)
            pltpu.make_async_copy(source.at[span], target.at[span], sem).start()

    spread_in[...] = jnp.zeros_like(spread_in)
    spread_out[...] = jnp.zeros_like(spread_out)
    loads["tokens"].wait()
    loads["norm_gain"].wait()
    normed_buf[...] = normalize(tokens[...], norm_gain[...])
    for name in ("log_step", "decay", "frequency"):
        loads[name].wait()
    coefficients(log_step[...], decay_rate[...], frequency[...], tables)
    loads["in_map"].wait()
    loads["out_map"].wait()
    sign = jnp.where(lax.broadcasted_iota(jnp.int32, (1, LANES), 1) < states, 1.0, -1.0)
    for group in range(groups):
        block, place = divmod(group, per_block)
        rows = slice(place * channels, (place + 1) * channels)
        columns = slice(place * LANES, (place + 1) * LANES)
        tile = slice(group * channels, (group + 1) * channels)
        spread_in[block, rows, columns] = in_map[tile, :]
        spread_out[block, rows, columns] = (out_map[tile, :].astype(jnp.float32) * sign).astype(
            jnp.bfloat16
        )
    total = None
    for part in range(in_parts):
        loads["w_in", part].wait()
        span = slice(part * width, (part + 1) * width)
        term = dot_wide(normed_buf[:, span], dense[:width, span])
        total = term if total is None else total + term
    drive = total.astype(jnp.bfloat16)
    loads["carried"].wait()
    loads["skip"].wait()
    weight_copies(gate_hbm, gate, weight_sem.at[0])
    weight_copies(up_hbm, up, weight_sem.at[0])
    for block in range(blocks):
        lanes = slice(block * LANES, (block + 1) * LANES)
        projected = dot_wide(drive[:, lanes], spread_in[block])
        for place in range(per_block):
            group = block * per_block + place
            columns = slice(place * LANES, (place + 1) * LANES)
            entry = projected[:, columns]
            old = carried[pl.ds(group, count_rows, stride=groups), :]
            straight = tables[0, group : group + 1, :] * old
            straight = straight + tables[2, group : group + 1, :] * entry
            cross = tables[1, group : group + 1, :] * old
            cross = cross + tables[3, group : group + 1, :] * entry
            new = straight + pltpu.roll(cross, states, 1)
            new_carried[pl.ds(group, count_rows, stride=groups), :] = new
            high = new.astype(jnp.bfloat16)
            joined[block, :count_rows, columns] = high
            joined[block, count_rows:, columns] = (new - high.astype(jnp.float32)).astype(
                jnp.bfloat16
            )
        both = dot_transposed(joined[block], spread_out[block])
        read = both[:count_rows] + both[count_rows:]
        read = read + skip[lanes].reshape(1, LANES) * drive[:, lanes].astype(jnp.float32)
        activated[:, lanes] = gelu(read).astype(jnp.bfloat16)

    def remote(source, target, send, recv, place):
        return pltpu.make_async_remote_copy(
            src_ref=source,
            dst_ref=target,
            send_sem=send,
            recv_sem=recv,
            device_id=place,
            device_id_type=MESH,
        )

    def exchange(part):
        return remote(
            partial.at[part], partial_in.at[part], partial_send, partial_recv.at[part], (ep, other)
        )

    for part in range(OUT_PARTS):
        span = slice(part * out_span, (part + 1) * out_span)
        loads["w_out", part].wait()
        partial[part] = dot_wide(activated[...], mix[:, span]).astype(jnp.bfloat16)
        if part == 0:
            pl.semaphore_wait(barrier, EXPERTS + group_size - 1)
        exchange(part).start()
    weight_copies(down_hbm, down, weight_sem.at[1])

    loads["ids"].wait()
    loads["logit"].wait()
    loads["expert_gain"].wait()
    pack, weighed = routing(ids[...], logit[...])
    pack = pack.astype(jnp.bfloat16)
    weighed = weighed.T
    weight_high = weighed.astype(jnp.bfloat16)
    weight_low = (weighed - weight_high.astype(jnp.float32)).astype(jnp.bfloat16)

    for part in range(OUT_PARTS):
        span = slice(part * out_span, (part + 1) * out_span)
        exchange(part).wait_recv()
        summed = partial[part].astype(jnp.float32) + partial_in[part].astype(jnp.float32)
        mixed_buf[:, span] = (tokens[:, span].astype(jnp.float32) + summed).astype(jnp.bfloat16)
    normed_buf[...] = normalize(mixed_buf[...], expert_gain[...])

    def direct(index, step):
        place = at_expert(step)
        return remote(
            packed.at[index, place],
            rows_buf.at[index, core, lane, expert],
            send_sem.at[0],
            direct_recv.at[index, step],
            (place * group_size + lane, core),
        )

    def to_peer(index, step, shift):
        source = at_expert(step)
        return remote(
            rows_buf.at[index, core, lane, source],
            rows_buf.at[index, core, lane, source],
            send_sem.at[1],
            peer_recv.at[index, shift],
            (expert * group_size + at_lane(shift), core),
        )

    def from_peer(index, shift):
        block = rows_buf.at[index, core, at_lane(-shift)]
        place = (expert * group_size + at_lane(shift), core)
        return remote(block, block, send_sem.at[1], peer_recv.at[index, shift], place)

    def across(index, shift):
        block = rows_buf.at[index, core, at_lane(-shift)]
        return remote(block, block, send_sem.at[2], core_recv.at[index], (ep, other))

    def from_core(index):
        block = rows_buf.at[index, other]
        return remote(block, block, send_sem.at[2], core_recv.at[index], (ep, other))

    for index in range(CHUNKS):
        columns = pl.ds(pl.multiple_of(core * half + index * chunk, LANES), chunk)
        chosen = dot_wide(pack, normed_buf[:, columns]).astype(jnp.bfloat16)
        packed[index] = chosen.reshape(EXPERTS, CAP, chunk)
        for step in SEND_ORDER:
            direct(index, step).start()
        rows_buf[index, core, lane, expert] = packed[index, expert]

    def relay(index):
        for step in WAIT_ORDER:
            if step:
                direct(index, step).wait_recv()
            for shift in range(1, group_size):
                to_peer(index, step, shift).start()
        across(index, 0).start()

    def cross(index):
        for shift in range(1, group_size):
            from_peer(index, shift).wait_recv()
            across(index, shift).start()

    height = hidden_units if hidden_units < 1024 else hidden_units // 2

    def accumulate(index):
        low = slice(index * chunk, (index + 1) * chunk)
        high = slice(half + index * chunk, half + (index + 1) * chunk)

        def part(number, carry):
            units = pl.ds(pl.multiple_of(number * height, 16), height)

            def project(weights):
                value = dot_transposed(
                    weights[units, low], rows_buf[index, 0].reshape(total_rows, chunk)
                )
                return value + dot_transposed(
                    weights[units, high], rows_buf[index, 1].reshape(total_rows, chunk)
                )

            gated = project(gate)
            upward = project(up)
            if index:
                gated = gate_sum[units, :] + gated
                upward = up_sum[units, :] + upward
            if index < CHUNKS - 1:
                gate_sum[units, :] = gated
                up_sum[units, :] = upward
            else:
                hidden_t[units, :] = (jax.nn.silu(gated) * upward).astype(jnp.bfloat16)
            return carry

        lax.fori_loop(0, hidden_units // height, part, 0)

    relay(0)
    for index in range(CHUNKS):
        if index + 1 < CHUNKS:
            relay(index + 1)
        cross(index)
        from_core(index).wait_recv()
        if index == 0:
            pltpu.make_async_copy(gate_up, gate_up, weight_sem.at[0]).wait()
        accumulate(index)
    for start in range(0, hidden_units, LANES):
        units = slice(start, min(start + LANES, hidden_units))
        hidden[:, units] = hidden_t[units, :].T
    pltpu.make_async_copy(down, down, weight_sem.at[1]).wait()

    def produce(owner, index):
        columns = pl.ds(pl.multiple_of(owner * half + index * piece, 128), piece)
        return jnp.dot(hidden[...], down[:, columns], preferred_element_type=jnp.float32)

    def swap(index):
        return remote(
            swap_out.at[index], swap_in.at[index], send_sem.at[3], swap_recv.at[index], (ep, other)
        )

    def sum_to_peer(index, shift):
        place = at_lane(shift)
        return remote(
            peer_out.at[index, place],
            peer_in.at[index, shift - 1],
            send_sem.at[4],
            sum_recv.at[index],
            (expert * group_size + place, core),
        )

    def from_peers(index):
        block = peer_in.at[index]
        return remote(block, block, send_sem.at[4], sum_recv.at[index], (ep, other))

    def give_back(index, step):
        place = at_expert(step)
        return remote(
            back_out.at[index, place],
            returned.at[index, expert],
            send_sem.at[5],
            back_recv.at[index],
            (place * group_size + lane, core),
        )

    def given_back(index):
        block = returned.at[index, : EXPERTS - 1]
        return remote(block, block, send_sem.at[5], back_recv.at[index], (ep, other))

    def start_swap(index):
        swap_out[index] = produce(other, index).astype(jnp.bfloat16)
        swap(index).start()

    start_swap(0)
    for index in range(PIECES):
        if index + 1 < PIECES:
            start_swap(index + 1)
        value = produce(core, index)
        swap(index).wait_recv()
        value = value + swap_in[index].astype(jnp.float32)
        value = value.reshape(group_size, EXPERTS, CAP, piece)
        own_sum[index] = value
        peer_out[index] = value.astype(jnp.bfloat16)
        for shift in range(1, group_size):
            sum_to_peer(index, shift).start()
    for index in range(PIECES):
        value = own_sum[index, lane]
        if group_size > 1:
            from_peers(index).wait_recv()
        for shift in range(1, group_size):
            value = value + peer_in[index, shift - 1].astype(jnp.float32)
        back_out[index] = value.astype(jnp.bfloat16)
        for step in BACK_ORDER:
            give_back(index, step).start()
        returned[index, expert] = back_out[index, expert]
    for index in range(PIECES):
        given_back(index).wait_recv()
        rows = returned[index].reshape(EXPERTS * CAP, piece)
        value = jnp.dot(weight_high, rows, preferred_element_type=jnp.float32)
        value = value + jnp.dot(weight_low, rows, preferred_element_type=jnp.float32)
        columns = pl.ds(pl.multiple_of(core * half + index * piece, 128), piece)
        value = value + mixed_buf[:, columns].astype(jnp.float32)
        out[:, index * piece : (index + 1) * piece] = value.astype(out.dtype)


    def sent(block, sem):
        remote(block, block, sem, sem, (ep, other)).wait_send()

    sent(partial, partial_send)
    sent(packed.at[:, : EXPERTS - 1], send_sem.at[0])
    if group_size > 1:
        sent(rows_buf.at[:, core, : group_size - 1], send_sem.at[1])
        sent(peer_out.at[:, : group_size - 1], send_sem.at[4])
    sent(rows_buf.at[:, core], send_sem.at[2])
    sent(swap_out, send_sem.at[3])
    sent(back_out.at[:, : EXPERTS - 1], send_sem.at[5])


def per_device(
    tokens,
    carried,
    decay_rate,
    frequency,
    log_step,
    in_map,
    out_map,
    skip_gain,
    norm_gain,
    w_in,
    w_out,
    expert_gain,
    route_ids,
    route_logit,
    w_gate,
    w_up,
    w_down,
):
    count_rows, model_width = tokens.shape
    groups, states = decay_rate.shape
    width = skip_gain.shape[0]
    per_block = LANES * groups // width
    blocks = groups // per_block
    sources = lax.axis_size("ep")
    group_size = sources // EXPERTS
    half = model_width // 2
    piece = half // PIECES
    chunk = half // CHUNKS
    hidden_units = w_down.shape[0]
    total_rows = sources * CAP
    peers = max(group_size - 1, 1)
    dma = pltpu.SemaphoreType.DMA
    narrow = jnp.bfloat16
    wide = jnp.float32
    vmem = pl.BlockSpec(memory_space=pltpu.VMEM)
    far = pl.BlockSpec(memory_space=pltpu.HBM)
    operands = (
        tokens,
        carried.reshape(count_rows * groups, 2 * states),
        decay_rate,
        frequency,
        log_step.reshape(1, groups),
        in_map.transpose(0, 2, 1).reshape(width, 2 * states),
        out_map.reshape(width, 2 * states),
        skip_gain,
        norm_gain.reshape(1, model_width),
        w_in,
        w_out,
        expert_gain.reshape(1, model_width),
        route_ids.T,
        route_logit.T,
        w_gate.T,
        w_up.T,
        w_down,
    )
    staged = operands[:9] + operands[11:14]
    new_tokens, new_carried = pl.pallas_call(
        functools.partial(layer_kernel, group_size),
        out_shape=(
            jax.ShapeDtypeStruct((count_rows, half), narrow),
            jax.ShapeDtypeStruct((count_rows * groups, 2 * states), wide),
        ),
        in_specs=[far] * len(operands),
        out_specs=(vmem, vmem),
        scratch_shapes=[pltpu.VMEM(value.shape, value.dtype) for value in staged]
        + [
            pltpu.VMEM((2, hidden_units, model_width), narrow),
            pltpu.VMEM((max(2 * width, hidden_units), model_width), narrow),
            pltpu.VMEM((4, groups, 2 * states), wide),
            pltpu.VMEM((blocks, LANES, per_block * LANES), narrow),
            pltpu.VMEM((blocks, LANES, per_block * LANES), narrow),
            pltpu.VMEM((blocks, 2 * count_rows, per_block * LANES), narrow),
            pltpu.VMEM((count_rows, width), narrow),
            pltpu.VMEM((OUT_PARTS, count_rows, model_width // OUT_PARTS), narrow),
            pltpu.VMEM((OUT_PARTS, count_rows, model_width // OUT_PARTS), narrow),
            pltpu.VMEM((count_rows, model_width), narrow),
            pltpu.VMEM((count_rows, model_width), narrow),
            pltpu.VMEM((CHUNKS, EXPERTS, CAP, chunk), narrow),
            pltpu.VMEM((CHUNKS, 2, group_size, EXPERTS, CAP, chunk), narrow),
            pltpu.VMEM((hidden_units, total_rows), wide),
            pltpu.VMEM((hidden_units, total_rows), wide),
            pltpu.VMEM((hidden_units, total_rows), narrow),
            pltpu.VMEM((total_rows, hidden_units), narrow),
            pltpu.VMEM((PIECES, total_rows, piece), narrow),
            pltpu.VMEM((PIECES, total_rows, piece), narrow),
            pltpu.VMEM((PIECES, group_size, EXPERTS, CAP, piece), wide),
            pltpu.VMEM((PIECES, group_size, EXPERTS, CAP, piece), narrow),
            pltpu.VMEM((PIECES, peers, EXPERTS, CAP, piece), narrow),
            pltpu.VMEM((PIECES, EXPERTS, CAP, piece), narrow),
            pltpu.VMEM((PIECES, EXPERTS, CAP, piece), narrow),
            dma((len(staged) + model_width // width + OUT_PARTS,)),
            dma((2,)),
            dma,
            dma((OUT_PARTS,)),
            dma((CHUNKS, EXPERTS)),
            dma((CHUNKS, group_size)),
            dma((CHUNKS,)),
            dma((PIECES,)),
            dma((PIECES,)),
            dma((PIECES,)),
            dma((6,)),
        ],
        compiler_params=pltpu.CompilerParams(
            collective_id=0, has_side_effects=True, vmem_limit_bytes=50 * 1024 * 1024
        ),
    )(*[pltpu.with_memory_space_constraint(value, pltpu.HBM) for value in operands])
    return (new_tokens, new_carried.reshape(count_rows, groups, 2 * states))


def solution(mesh):
    return jax.shard_map(
        per_device,
        mesh=mesh,
        in_specs=(
            P("ep", None),
            P("ep", "tp", None),
            P("tp", None),
            P("tp", None),
            P("tp"),
            P("tp", None, None),
            P("tp", None, None),
            P("tp"),
            P(),
            P(None, "tp"),
            P("tp", None),
            P(),
            P("ep", None),
            P("ep", None),
            P(None, ("ep", "tp")),
            P(None, ("ep", "tp")),
            P(("ep", "tp"), None),
        ),
        out_specs=(P("ep", "tp"), P("ep", "tp", None)),
        check_vma=False,
    )
```

```python
import functools

import jax
import jax.numpy as jnp
from jax import lax
from jax.experimental import pallas as pl
from jax.experimental.pallas import tpu as pltpu
from jax.sharding import PartitionSpec as P

EXPERTS = 8
TOP = 2
CAP = 16

MESH = pl.DeviceIdType.MESH
SEND_ORDER = (1, 3, 2, 5, 4, 7, 6)
WAIT_ORDER = (0, 1, 2, 3, 4, 5, 6, 7)
BACK_ORDER = (4, 6, 5, 7, 2, 3, 1)
CHUNK_SHARES = (3, 3)
PIECE_SHARES = (2, 2, 2)
STRIP = 256
UNIT_PARTS = 2
LANES = 128
LATE_PART = 1
OUT_PARTS = 4
WEIGHT_PARTS = 3


def parts_of(length, shares):
    unit = length // sum(shares)
    starts = [unit * sum(shares[:index]) for index in range(len(shares))]
    return [(start, unit * share) for start, share in zip(starts, shares)]


def normalize(rows, gain):
    wide = rows.astype(jnp.float32)
    scaled = wide * lax.rsqrt(jnp.mean(wide * wide, axis=-1, keepdims=True) + 1e-06)
    return (scaled * gain).astype(jnp.bfloat16)


def dot_wide(left, right):
    return jnp.dot(left, right, preferred_element_type=jnp.float32)


def dot_transposed(left, right):
    return lax.dot_general(
        left, right, (((1,), (1,)), ((), ())), preferred_element_type=jnp.float32
    )


def gelu(value):
    inner = 0.7978845608028654 * (value + 0.044715 * (value * value * value))
    return value * (0.5 * (1.0 + jnp.tanh(inner)))


def coefficients(log_step, decay_rate, frequency, tables):
    groups, half = decay_rate.shape
    row = lax.broadcasted_iota(jnp.int32, (groups, groups), 0)
    column = lax.broadcasted_iota(jnp.int32, (groups, groups), 1)
    spread = jnp.where(row == column, jnp.broadcast_to(log_step, (groups, groups)), 0.0)
    step_size = jnp.exp(jnp.sum(spread, axis=1, keepdims=True))
    magnitude = jnp.exp(-decay_rate * step_size)
    real_decay = magnitude * jnp.cos(frequency * step_size)
    imag_decay = magnitude * jnp.sin(frequency * step_size)
    denom = decay_rate * decay_rate + frequency * frequency
    real_less = real_decay - 1.0
    real_factor = (-real_less * decay_rate + imag_decay * frequency) / denom
    imag_factor = (-imag_decay * decay_rate - real_less * frequency) / denom
    tables[0] = jnp.concatenate([real_decay, real_decay], axis=1)
    tables[1] = jnp.concatenate([imag_decay, -imag_decay], axis=1)
    tables[2] = jnp.concatenate([real_factor, real_factor], axis=1)
    tables[3] = jnp.concatenate([imag_factor, -imag_factor], axis=1)


def routing(ids, logit):
    count_rows = ids.shape[1]
    expert = lax.broadcasted_iota(jnp.int32, (EXPERTS, count_rows), 0)
    first = (ids[0:1, :] == expert).astype(jnp.float32)
    second = (ids[1:2, :] == expert).astype(jnp.float32)
    named = first + second
    weight = first * jax.nn.sigmoid(logit[0:1, :] - logit[1:2, :])
    weight = weight + second * jax.nn.sigmoid(logit[1:2, :] - logit[0:1, :])
    row = lax.broadcasted_iota(jnp.int32, (count_rows, count_rows), 0)
    column = lax.broadcasted_iota(jnp.int32, (count_rows, count_rows), 1)
    earlier = dot_wide(named, (row < column).astype(jnp.float32))
    slots = (EXPERTS, CAP, count_rows)
    slot = lax.broadcasted_iota(jnp.int32, slots, 1).astype(jnp.float32)
    here = slot == jnp.broadcast_to(earlier[:, None, :], slots)
    pack = jnp.where(here, jnp.broadcast_to(named[:, None, :], slots), 0.0)
    weighed = jnp.where(here, jnp.broadcast_to(weight[:, None, :], slots), 0.0)
    total = EXPERTS * CAP
    return pack.reshape(total, count_rows), weighed.reshape(total, count_rows)


def layer_kernel(
    group_size,
    tokens_hbm,
    carried_hbm,
    decay_hbm,
    frequency_hbm,
    log_step_hbm,
    in_map_hbm,
    out_map_hbm,
    skip_hbm,
    norm_gain_hbm,
    w_in_hbm,
    w_out_hbm,
    expert_gain_hbm,
    ids_hbm,
    logit_hbm,
    gate_hbm,
    up_hbm,
    down_hbm,
    out,
    new_carried,
    tokens,
    carried,
    decay_rate,
    frequency,
    log_step,
    in_map,
    out_map,
    skip,
    norm_gain,
    expert_gain,
    ids,
    logit,
    gate_up,
    dense,
    tables,
    spread_in,
    spread_out,
    joined,
    activated,
    partial,
    partial_in,
    mixed_buf,
    normed_buf,
    packed,
    rows_buf,
    gate_sum,
    up_sum,
    hidden_t,
    hidden,
    swap_out,
    swap_in,
    own_sum,
    peer_out,
    peer_in,
    back_out,
    returned,
    load_sem,
    weight_sem,
    partial_send,
    partial_recv,
    direct_send,
    direct_recv,
    peer_send,
    peer_recv,
    core_send,
    core_recv,
    swap_send,
    swap_recv,
    sum_send,
    sum_recv,
    back_send,
    back_recv,
):
    ep = lax.axis_index("ep")
    core = lax.axis_index("tp")
    expert = ep // group_size
    lane = ep % group_size
    other = 1 - core
    count_rows, model_width = tokens.shape
    groups, states = decay_rate.shape
    width = skip.shape[0]
    channels = width // groups
    per_block = LANES // channels
    blocks = groups // per_block
    half = model_width // 2
    hidden_units = gate_hbm.shape[0]
    total_rows = group_size * EXPERTS * CAP
    in_parts = model_width // width
    gate, up = gate_up.at[0], gate_up.at[1]
    mix = dense.at[width : 2 * width]
    down = dense.at[:hidden_units]
    pieces = parts_of(half, PIECE_SHARES)
    strips = half // STRIP
    chunks = parts_of(half, CHUNK_SHARES)

    def at_expert(step):
        place, bit = 0, 1
        while bit < EXPERTS:
            place = place + bit * lax.rem(expert // bit + step // bit, 2)
            bit *= 2
        return place

    def at_lane(step):
        return lax.rem(lane + step + group_size, group_size)

    loads = {}

    def load(name, source, target):
        loads[name] = pltpu.make_async_copy(source, target, load_sem.at[len(loads)])
        loads[name].start()

    load("tokens", tokens_hbm, tokens)
    load("norm_gain", norm_gain_hbm, norm_gain)
    for part in range(in_parts):
        span = pl.ds(part * width, width)
        load(("w_in", part), w_in_hbm.at[span], dense.at[:width, span])
    load("log_step", log_step_hbm, log_step)
    load("decay", decay_hbm, decay_rate)
    load("frequency", frequency_hbm, frequency)
    load("in_map", in_map_hbm, in_map)
    load("out_map", out_map_hbm, out_map)
    load("carried", carried_hbm, carried)
    load("skip", skip_hbm, skip)
    load("ids", ids_hbm, ids)
    load("logit", logit_hbm, logit)
    load("expert_gain", expert_gain_hbm, expert_gain)
    out_span = model_width // OUT_PARTS

    barrier = pltpu.get_barrier_semaphore()
    pl.semaphore_signal(barrier, inc=1, device_id=(ep, other), device_id_type=MESH)
    for step in range(1, EXPERTS):
        target = at_expert(step) * group_size + lane
        pl.semaphore_signal(barrier, inc=1, device_id=(target, core), device_id_type=MESH)
    for step in range(1, group_size):
        target = expert * group_size + at_lane(step)
        pl.semaphore_signal(barrier, inc=1, device_id=(target, core), device_id_type=MESH)

    weight_span = hidden_units // WEIGHT_PARTS

    def weight_copies(source, target, sem):
        for part in range(WEIGHT_PARTS):
            span = pl.ds(part * weight_span, weight_span)
            pltpu.make_async_copy(source.at[span], target.at[span], sem).start()

    spread_in[...] = jnp.zeros_like(spread_in)
    spread_out[...] = jnp.zeros_like(spread_out)
    loads["tokens"].wait()
    loads["norm_gain"].wait()
    normed_buf[...] = normalize(tokens[...], norm_gain[...])
    for name in ("log_step", "decay", "frequency"):
        loads[name].wait()
    coefficients(log_step[...], decay_rate[...], frequency[...], tables)
    loads["in_map"].wait()
    loads["out_map"].wait()
    sign = jnp.where(lax.broadcasted_iota(jnp.int32, (1, LANES), 1) < states, 1.0, -1.0)
    for group in range(groups):
        block, place = divmod(group, per_block)
        rows = slice(place * channels, (place + 1) * channels)
        columns = slice(place * LANES, (place + 1) * LANES)
        tile = slice(group * channels, (group + 1) * channels)
        spread_in[block, rows, columns] = in_map[tile, :]
        spread_out[block, rows, columns] = (out_map[tile, :].astype(jnp.float32) * sign).astype(
            jnp.bfloat16
        )
    total = None
    for part in range(in_parts):
        loads["w_in", part].wait()
        if part == LATE_PART:
            for late in range(OUT_PARTS):
                span = pl.ds(late * out_span, out_span)
                load(("w_out", late), w_out_hbm.at[:, span], mix.at[:, span])
        span = slice(part * width, (part + 1) * width)
        term = dot_wide(normed_buf[:, span], dense[:width, span])
        total = term if total is None else total + term
    drive = total.astype(jnp.bfloat16)
    loads["carried"].wait()
    loads["skip"].wait()
    weight_copies(gate_hbm, gate, weight_sem.at[0])
    weight_copies(up_hbm, up, weight_sem.at[0])
    for block in range(blocks):
        lanes = slice(block * LANES, (block + 1) * LANES)
        projected = dot_wide(drive[:, lanes], spread_in[block])
        for place in range(per_block):
            group = block * per_block + place
            columns = slice(place * LANES, (place + 1) * LANES)
            entry = projected[:, columns]
            old = carried[pl.ds(group, count_rows, stride=groups), :]
            straight = tables[0, group : group + 1, :] * old
            straight = straight + tables[2, group : group + 1, :] * entry
            cross = tables[1, group : group + 1, :] * old
            cross = cross + tables[3, group : group + 1, :] * entry
            new = straight + pltpu.roll(cross, states, 1)
            new_carried[pl.ds(group, count_rows, stride=groups), :] = new
            high = new.astype(jnp.bfloat16)
            joined[block, :count_rows, columns] = high
            joined[block, count_rows:, columns] = (new - high.astype(jnp.float32)).astype(
                jnp.bfloat16
            )
        both = dot_transposed(joined[block], spread_out[block])
        read = both[:count_rows] + both[count_rows:]
        read = read + skip[lanes].reshape(1, LANES) * drive[:, lanes].astype(jnp.float32)
        activated[:, lanes] = gelu(read).astype(jnp.bfloat16)

    def remote(source, target, send, recv, place):
        return pltpu.make_async_remote_copy(
            src_ref=source,
            dst_ref=target,
            send_sem=send,
            recv_sem=recv,
            device_id=place,
            device_id_type=MESH,
        )

    def exchange(part):
        return remote(
            partial.at[part], partial_in.at[part], partial_send, partial_recv.at[part], (ep, other)
        )

    for part in range(OUT_PARTS):
        span = slice(part * out_span, (part + 1) * out_span)
        loads["w_out", part].wait()
        partial[part] = dot_wide(activated[...], mix[:, span]).astype(jnp.bfloat16)
        if part == 0:
            pl.semaphore_wait(barrier, EXPERTS + group_size - 1)
        exchange(part).start()
    weight_copies(down_hbm, down, weight_sem.at[1])

    loads["ids"].wait()
    loads["logit"].wait()
    loads["expert_gain"].wait()
    pack, weighed = routing(ids[...], logit[...])
    pack = pack.astype(jnp.bfloat16)
    weighed = weighed.T
    weight_high = weighed.astype(jnp.bfloat16)
    weight_low = (weighed - weight_high.astype(jnp.float32)).astype(jnp.bfloat16)

    for part in range(OUT_PARTS):
        span = slice(part * out_span, (part + 1) * out_span)
        exchange(part).wait_recv()
        summed = partial[part].astype(jnp.float32) + partial_in[part].astype(jnp.float32)
        mixed_buf[:, span] = (tokens[:, span].astype(jnp.float32) + summed).astype(jnp.bfloat16)
    normed_buf[...] = normalize(mixed_buf[...], expert_gain[...])

    def direct(index, step):
        place = at_expert(step)
        return remote(
            packed[index].at[place],
            rows_buf[index].at[core, lane, expert],
            direct_send.at[index],
            direct_recv.at[index, step],
            (place * group_size + lane, core),
        )

    def to_peer(index, step, shift):
        block = rows_buf[index].at[core, lane, at_expert(step)]
        place = (expert * group_size + at_lane(shift), core)
        return remote(block, block, peer_send.at[index], peer_recv.at[index, shift], place)

    def from_peer(index, shift):
        block = rows_buf[index].at[core, at_lane(-shift)]
        place = (expert * group_size + at_lane(shift), core)
        return remote(block, block, peer_send.at[index], peer_recv.at[index, shift], place)

    def across(index, shift):
        block = rows_buf[index].at[core, at_lane(-shift)]
        return remote(block, block, core_send.at[index], core_recv.at[index], (ep, other))

    def from_core(index):
        block = rows_buf[index].at[other]
        return remote(block, block, core_send.at[index], core_recv.at[index], (ep, other))

    for index, (begin, size) in enumerate(chunks):
        columns = pl.ds(pl.multiple_of(core * half + begin, LANES), size)
        chosen = dot_wide(pack, normed_buf[:, columns]).astype(jnp.bfloat16)
        packed[index][...] = chosen.reshape(EXPERTS, CAP, size)
        for step in SEND_ORDER:
            direct(index, step).start()
        rows_buf[index][core, lane, expert] = packed[index][expert]

    def relay(index):
        for step in WAIT_ORDER:
            if step:
                direct(index, step).wait_recv()
            for shift in range(1, group_size):
                to_peer(index, step, shift).start()
        across(index, 0).start()

    def cross(index):
        for shift in range(1, group_size):
            from_peer(index, shift).wait_recv()
            across(index, shift).start()

    height = hidden_units // UNIT_PARTS

    def accumulate(index, number):
        begin, size = chunks[index]
        units = slice(number * height, (number + 1) * height)
        arrived = rows_buf[index]

        def project(weights):
            value = dot_transposed(
                weights[units, begin : begin + size], arrived[0].reshape(total_rows, size)
            )
            return value + dot_transposed(
                weights[units, half + begin : half + begin + size],
                arrived[1].reshape(total_rows, size),
            )

        gated = project(gate)
        upward = project(up)
        if index:
            gated = gate_sum[units, :] + gated
            upward = up_sum[units, :] + upward
        if index < len(chunks) - 1:
            gate_sum[units, :] = gated
            up_sum[units, :] = upward
        else:
            hidden_t[units, :] = (jax.nn.silu(gated) * upward).astype(jnp.bfloat16)

    def transpose(begin, end):
        for start in range(begin, end, LANES):
            units = slice(start, min(start + LANES, end))
            hidden[:, units] = hidden_t[units, :].T

    relay(0)
    for index in range(len(chunks)):
        if index + 1 < len(chunks):
            relay(index + 1)
        if index == 0:
            cross(0)
            pltpu.make_async_copy(gate_up, gate_up, weight_sem.at[0]).wait()
        from_core(index).wait_recv()
        for number in range(UNIT_PARTS):
            accumulate(index, number)
            if number == 0 and index + 1 < len(chunks):
                cross(index + 1)
    transpose(0, hidden_units)
    pltpu.make_async_copy(down, down, weight_sem.at[1]).wait()

    def produce(owner, index):
        begin, size = pieces[index]
        columns = pl.ds(pl.multiple_of(owner * half + begin, LANES), size)
        return jnp.dot(hidden[...], down[:, columns], preferred_element_type=jnp.float32)

    def swap(index):
        return remote(
            swap_out[index], swap_in[index], swap_send.at[index], swap_recv.at[index], (ep, other)
        )

    def sum_to_peer(index, shift):
        place = at_lane(shift)
        return remote(
            peer_out.at[index, place],
            peer_in.at[index, shift - 1],
            sum_send,
            sum_recv.at[index],
            (expert * group_size + place, core),
        )

    def from_peers(index):
        block = peer_in.at[index]
        return remote(block, block, sum_send, sum_recv.at[index], (ep, other))

    def give_back(index, step):
        place = at_expert(step)
        return remote(
            back_out.at[index, place],
            returned.at[index, expert],
            back_send,
            back_recv.at[index],
            (place * group_size + lane, core),
        )

    def given_back(index):
        block = returned.at[index, : EXPERTS - 1]
        return remote(block, block, back_send, back_recv.at[index], (ep, other))

    def start_swap(index):
        swap_out[index][...] = produce(other, index).astype(jnp.bfloat16)
        swap(index).start()

    start_swap(0)
    for index, (begin, size) in enumerate(pieces):
        if index + 1 < len(pieces):
            start_swap(index + 1)
        value = produce(core, index)
        swap(index).wait_recv()
        value = value + swap_in[index][...].astype(jnp.float32)
        for inner in range(0, size, STRIP):
            strip = (begin + inner) // STRIP
            shape = (group_size, EXPERTS, CAP, STRIP)
            columns = value[:, inner : inner + STRIP].reshape(shape)
            own_sum[strip] = columns
            peer_out[strip] = columns.astype(jnp.bfloat16)
            for shift in range(1, group_size):
                sum_to_peer(strip, shift).start()
    for index in range(strips):
        value = own_sum[index, lane]
        if group_size > 1:
            from_peers(index).wait_recv()
        for shift in range(1, group_size):
            value = value + peer_in[index, shift - 1].astype(jnp.float32)
        back_out[index] = value.astype(jnp.bfloat16)
        for step in BACK_ORDER:
            give_back(index, step).start()
        returned[index, expert] = back_out[index, expert]
    for index in range(strips):
        given_back(index).wait_recv()
        rows = returned[index].reshape(EXPERTS * CAP, STRIP)
        value = jnp.dot(weight_high, rows, preferred_element_type=jnp.float32)
        value = value + jnp.dot(weight_low, rows, preferred_element_type=jnp.float32)
        columns = pl.ds(pl.multiple_of(core * half + index * STRIP, LANES), STRIP)
        value = value + mixed_buf[:, columns].astype(jnp.float32)
        out[:, index * STRIP : (index + 1) * STRIP] = value.astype(out.dtype)

    def sent(block, sem):
        remote(block, block, sem, sem, (ep, other)).wait_send()

    sent(partial, partial_send)
    for index in range(len(chunks)):
        sent(packed[index].at[: EXPERTS - 1], direct_send.at[index])
        if group_size > 1:
            sent(rows_buf[index].at[core, : group_size - 1], peer_send.at[index])
        sent(rows_buf[index].at[core], core_send.at[index])
    for index in range(len(pieces)):
        sent(swap_out[index], swap_send.at[index])
    if group_size > 1:
        sent(peer_out.at[:, : group_size - 1], sum_send)
    sent(back_out.at[:, : EXPERTS - 1], back_send)


def per_device(
    tokens,
    carried,
    decay_rate,
    frequency,
    log_step,
    in_map,
    out_map,
    skip_gain,
    norm_gain,
    w_in,
    w_out,
    expert_gain,
    route_ids,
    route_logit,
    w_gate,
    w_up,
    w_down,
):
    count_rows, model_width = tokens.shape
    groups, states = decay_rate.shape
    width = skip_gain.shape[0]
    per_block = LANES * groups // width
    blocks = groups // per_block
    sources = lax.axis_size("ep")
    group_size = sources // EXPERTS
    half = model_width // 2
    pieces = parts_of(half, PIECE_SHARES)
    strips = half // STRIP
    chunks = parts_of(half, CHUNK_SHARES)
    hidden_units = w_down.shape[0]
    total_rows = sources * CAP
    peers = max(group_size - 1, 1)
    dma = pltpu.SemaphoreType.DMA
    narrow = jnp.bfloat16
    wide = jnp.float32
    vmem = pl.BlockSpec(memory_space=pltpu.VMEM)
    far = pl.BlockSpec(memory_space=pltpu.HBM)
    operands = (
        tokens,
        carried.reshape(count_rows * groups, 2 * states),
        decay_rate,
        frequency,
        log_step.reshape(1, groups),
        in_map.transpose(0, 2, 1).reshape(width, 2 * states),
        out_map.reshape(width, 2 * states),
        skip_gain,
        norm_gain.reshape(1, model_width),
        w_in,
        w_out,
        expert_gain.reshape(1, model_width),
        route_ids.T,
        route_logit.T,
        w_gate.T,
        w_up.T,
        w_down,
    )
    staged = operands[:9] + operands[11:14]

    def each(parts, shape, dtype=narrow):
        return tuple(pltpu.VMEM((*shape, size), dtype) for _, size in parts)

    new_tokens, new_carried = pl.pallas_call(
        functools.partial(layer_kernel, group_size),
        out_shape=(
            jax.ShapeDtypeStruct((count_rows, half), narrow),
            jax.ShapeDtypeStruct((count_rows * groups, 2 * states), wide),
        ),
        in_specs=[far] * len(operands),
        out_specs=(vmem, vmem),
        scratch_shapes=[pltpu.VMEM(value.shape, value.dtype) for value in staged]
        + [
            pltpu.VMEM((2, hidden_units, model_width), narrow),
            pltpu.VMEM((max(2 * width, hidden_units), model_width), narrow),
            pltpu.VMEM((4, groups, 2 * states), wide),
            pltpu.VMEM((blocks, LANES, per_block * LANES), narrow),
            pltpu.VMEM((blocks, LANES, per_block * LANES), narrow),
            pltpu.VMEM((blocks, 2 * count_rows, per_block * LANES), narrow),
            pltpu.VMEM((count_rows, width), narrow),
            pltpu.VMEM((OUT_PARTS, count_rows, model_width // OUT_PARTS), narrow),
            pltpu.VMEM((OUT_PARTS, count_rows, model_width // OUT_PARTS), narrow),
            pltpu.VMEM((count_rows, model_width), narrow),
            pltpu.VMEM((count_rows, model_width), narrow),
            each(chunks, (EXPERTS, CAP)),
            each(chunks, (2, group_size, EXPERTS, CAP)),
            pltpu.VMEM((hidden_units, total_rows), wide),
            pltpu.VMEM((hidden_units, total_rows), wide),
            pltpu.VMEM((hidden_units, total_rows), narrow),
            pltpu.VMEM((total_rows, hidden_units), narrow),
            each(pieces, (total_rows,)),
            each(pieces, (total_rows,)),
            pltpu.VMEM((strips, group_size, EXPERTS, CAP, STRIP), wide),
            pltpu.VMEM((strips, group_size, EXPERTS, CAP, STRIP), narrow),
            pltpu.VMEM((strips, peers, EXPERTS, CAP, STRIP), narrow),
            pltpu.VMEM((strips, EXPERTS, CAP, STRIP), narrow),
            pltpu.VMEM((strips, EXPERTS, CAP, STRIP), narrow),
            dma((len(staged) + model_width // width + OUT_PARTS,)),
            dma((2,)),
            dma,
            dma((OUT_PARTS,)),
            dma((len(chunks),)),
            dma((len(chunks), EXPERTS)),
            dma((len(chunks),)),
            dma((len(chunks), group_size)),
            dma((len(chunks),)),
            dma((len(chunks),)),
            dma((len(pieces),)),
            dma((len(pieces),)),
            dma,
            dma((strips,)),
            dma,
            dma((strips,)),
        ],
        compiler_params=pltpu.CompilerParams(
            collective_id=0, has_side_effects=True, vmem_limit_bytes=50 * 1024 * 1024
        ),
    )(*[pltpu.with_memory_space_constraint(value, pltpu.HBM) for value in operands])
    return (new_tokens, new_carried.reshape(count_rows, groups, 2 * states))


def solution(mesh):
    return jax.shard_map(
        per_device,
        mesh=mesh,
        in_specs=(
            P("ep", None),
            P("ep", "tp", None),
            P("tp", None),
            P("tp", None),
            P("tp"),
            P("tp", None, None),
            P("tp", None, None),
            P("tp"),
            P(),
            P(None, "tp"),
            P("tp", None),
            P(),
            P("ep", None),
            P("ep", None),
            P(None, ("ep", "tp")),
            P(None, ("ep", "tp")),
            P(("ep", "tp"), None),
        ),
        out_specs=(P("ep", "tp"), P("ep", "tp", None)),
        check_vma=False,
    )
```

```python
import functools

import jax
import jax.numpy as jnp
from jax import lax
from jax.experimental import pallas as pl
from jax.experimental.pallas import tpu as pltpu
from jax.sharding import PartitionSpec as P

EXPERTS = 8
TOP = 2
CAP = 16

MESH = pl.DeviceIdType.MESH
SEND_ORDER = (1, 3, 2, 5, 4, 7, 6)
WAIT_ORDER = (0, 1, 2, 3, 4, 5, 6, 7)
BACK_ORDER = (4, 6, 5, 7, 2, 3, 1)
CHUNK_SHARES = (3, 3)
PIECE_SHARES = (2, 2, 2)
STRIP = 256
UNIT_PARTS = 2
LANES = 128
LATE_PART = 1
OUT_PARTS = 2
WEIGHT_PARTS = 3


def parts_of(length, shares):
    unit = length // sum(shares)
    starts = [unit * sum(shares[:index]) for index in range(len(shares))]
    return [(start, unit * share) for start, share in zip(starts, shares)]


def normalize(rows, gain):
    wide = rows.astype(jnp.float32)
    scaled = wide * lax.rsqrt(jnp.mean(wide * wide, axis=-1, keepdims=True) + 1e-06)
    return (scaled * gain).astype(jnp.bfloat16)


def dot_wide(left, right):
    return jnp.dot(left, right, preferred_element_type=jnp.float32)


def dot_transposed(left, right):
    return lax.dot_general(
        left, right, (((1,), (1,)), ((), ())), preferred_element_type=jnp.float32
    )


def gelu(value):
    inner = 0.7978845608028654 * (value + 0.044715 * (value * value * value))
    return value * (0.5 * (1.0 + jnp.tanh(inner)))


def coefficients(log_step, decay_rate, frequency, tables):
    groups, half = decay_rate.shape
    row = lax.broadcasted_iota(jnp.int32, (groups, groups), 0)
    column = lax.broadcasted_iota(jnp.int32, (groups, groups), 1)
    spread = jnp.where(row == column, jnp.broadcast_to(log_step, (groups, groups)), 0.0)
    step_size = jnp.exp(jnp.sum(spread, axis=1, keepdims=True))
    magnitude = jnp.exp(-decay_rate * step_size)
    real_decay = magnitude * jnp.cos(frequency * step_size)
    imag_decay = magnitude * jnp.sin(frequency * step_size)
    denom = decay_rate * decay_rate + frequency * frequency
    real_less = real_decay - 1.0
    real_factor = (-real_less * decay_rate + imag_decay * frequency) / denom
    imag_factor = (-imag_decay * decay_rate - real_less * frequency) / denom
    tables[0] = jnp.concatenate([real_decay, real_decay], axis=1)
    tables[1] = jnp.concatenate([imag_decay, -imag_decay], axis=1)
    tables[2] = jnp.concatenate([real_factor, real_factor], axis=1)
    tables[3] = jnp.concatenate([imag_factor, -imag_factor], axis=1)


def routing(ids, logit):
    count_rows = ids.shape[1]
    expert = lax.broadcasted_iota(jnp.int32, (EXPERTS, count_rows), 0)
    first = (ids[0:1, :] == expert).astype(jnp.float32)
    second = (ids[1:2, :] == expert).astype(jnp.float32)
    named = first + second
    weight = first * jax.nn.sigmoid(logit[0:1, :] - logit[1:2, :])
    weight = weight + second * jax.nn.sigmoid(logit[1:2, :] - logit[0:1, :])
    row = lax.broadcasted_iota(jnp.int32, (count_rows, count_rows), 0)
    column = lax.broadcasted_iota(jnp.int32, (count_rows, count_rows), 1)
    earlier = dot_wide(named, (row < column).astype(jnp.float32))
    slots = (EXPERTS, CAP, count_rows)
    slot = lax.broadcasted_iota(jnp.int32, slots, 1).astype(jnp.float32)
    here = slot == jnp.broadcast_to(earlier[:, None, :], slots)
    pack = jnp.where(here, jnp.broadcast_to(named[:, None, :], slots), 0.0)
    weighed = jnp.where(here, jnp.broadcast_to(weight[:, None, :], slots), 0.0)
    total = EXPERTS * CAP
    return pack.reshape(total, count_rows), weighed.reshape(total, count_rows)


def layer_kernel(
    group_size,
    tokens_hbm,
    carried_hbm,
    decay_hbm,
    frequency_hbm,
    log_step_hbm,
    in_map_hbm,
    out_map_hbm,
    skip_hbm,
    norm_gain_hbm,
    w_in_hbm,
    w_out_hbm,
    expert_gain_hbm,
    ids_hbm,
    logit_hbm,
    gate_hbm,
    up_hbm,
    down_hbm,
    out,
    new_carried,
    tokens,
    carried,
    decay_rate,
    frequency,
    log_step,
    in_map,
    out_map,
    skip,
    norm_gain,
    expert_gain,
    ids,
    logit,
    gate_up,
    dense,
    tables,
    spread_in,
    spread_out,
    joined,
    activated,
    partial,
    partial_in,
    mixed_buf,
    normed_buf,
    packed,
    rows_buf,
    gate_sum,
    up_sum,
    hidden_t,
    hidden,
    swap_out,
    swap_in,
    own_sum,
    peer_out,
    peer_in,
    back_out,
    returned,
    load_sem,
    weight_sem,
    partial_send,
    partial_recv,
    direct_send,
    direct_recv,
    peer_send,
    peer_recv,
    core_send,
    core_recv,
    swap_send,
    swap_recv,
    sum_send,
    sum_recv,
    back_send,
    back_recv,
):
    ep = lax.axis_index("ep")
    core = lax.axis_index("tp")
    expert = ep // group_size
    lane = ep % group_size
    other = 1 - core
    count_rows, model_width = tokens.shape
    groups, states = decay_rate.shape
    width = skip.shape[0]
    channels = width // groups
    per_block = LANES // channels
    blocks = groups // per_block
    half = model_width // 2
    hidden_units = gate_hbm.shape[0]
    total_rows = group_size * EXPERTS * CAP
    in_parts = model_width // width
    gate, up = gate_up.at[0], gate_up.at[1]
    mix = dense.at[width : 2 * width]
    down = dense.at[:hidden_units]
    pieces = parts_of(half, PIECE_SHARES)
    strips = half // STRIP
    chunks = parts_of(half, CHUNK_SHARES)

    def at_expert(step):
        place, bit = 0, 1
        while bit < EXPERTS:
            place = place + bit * lax.rem(expert // bit + step // bit, 2)
            bit *= 2
        return place

    def at_lane(step):
        return lax.rem(lane + step + group_size, group_size)

    loads = {}

    def load(name, source, target):
        loads[name] = pltpu.make_async_copy(source, target, load_sem.at[len(loads)])
        loads[name].start()

    load("tokens", tokens_hbm, tokens)
    load("norm_gain", norm_gain_hbm, norm_gain)
    for part in range(in_parts):
        span = pl.ds(part * width, width)
        load(("w_in", part), w_in_hbm.at[span], dense.at[:width, span])
    load("log_step", log_step_hbm, log_step)
    load("decay", decay_hbm, decay_rate)
    load("frequency", frequency_hbm, frequency)
    load("in_map", in_map_hbm, in_map)
    load("out_map", out_map_hbm, out_map)
    load("carried", carried_hbm, carried)
    load("skip", skip_hbm, skip)
    load("ids", ids_hbm, ids)
    load("logit", logit_hbm, logit)
    load("expert_gain", expert_gain_hbm, expert_gain)
    out_span = model_width // OUT_PARTS

    barrier = pltpu.get_barrier_semaphore()
    pl.semaphore_signal(barrier, inc=1, device_id=(ep, other), device_id_type=MESH)
    for step in range(1, EXPERTS):
        target = at_expert(step) * group_size + lane
        pl.semaphore_signal(barrier, inc=1, device_id=(target, core), device_id_type=MESH)
    for step in range(1, group_size):
        target = expert * group_size + at_lane(step)
        pl.semaphore_signal(barrier, inc=1, device_id=(target, core), device_id_type=MESH)

    weight_span = hidden_units // WEIGHT_PARTS

    def weight_copies(source, target, sem):
        for part in range(WEIGHT_PARTS):
            span = pl.ds(part * weight_span, weight_span)
            pltpu.make_async_copy(source.at[span], target.at[span], sem).start()

    spread_in[...] = jnp.zeros_like(spread_in)
    spread_out[...] = jnp.zeros_like(spread_out)
    loads["tokens"].wait()
    loads["norm_gain"].wait()
    normed_buf[...] = normalize(tokens[...], norm_gain[...])
    for name in ("log_step", "decay", "frequency"):
        loads[name].wait()
    coefficients(log_step[...], decay_rate[...], frequency[...], tables)
    loads["in_map"].wait()
    loads["out_map"].wait()
    sign = jnp.where(lax.broadcasted_iota(jnp.int32, (1, LANES), 1) < states, 1.0, -1.0)
    for group in range(groups):
        block, place = divmod(group, per_block)
        rows = slice(place * channels, (place + 1) * channels)
        columns = slice(place * LANES, (place + 1) * LANES)
        tile = slice(group * channels, (group + 1) * channels)
        spread_in[block, rows, columns] = in_map[tile, :]
        spread_out[block, rows, columns] = (out_map[tile, :].astype(jnp.float32) * sign).astype(
            jnp.bfloat16
        )
    total = None
    for part in range(in_parts):
        loads["w_in", part].wait()
        if part == LATE_PART:
            for late in range(OUT_PARTS):
                span = pl.ds(late * out_span, out_span)
                load(("w_out", late), w_out_hbm.at[:, span], mix.at[:, span])
        span = slice(part * width, (part + 1) * width)
        term = dot_wide(normed_buf[:, span], dense[:width, span])
        total = term if total is None else total + term
    drive = total.astype(jnp.bfloat16)
    loads["carried"].wait()
    loads["skip"].wait()
    weight_copies(gate_hbm, gate, weight_sem.at[0])
    weight_copies(up_hbm, up, weight_sem.at[0])
    for block in range(blocks):
        lanes = slice(block * LANES, (block + 1) * LANES)
        projected = dot_wide(drive[:, lanes], spread_in[block])
        for place in range(per_block):
            group = block * per_block + place
            columns = slice(place * LANES, (place + 1) * LANES)
            entry = projected[:, columns]
            old = carried[pl.ds(group, count_rows, stride=groups), :]
            straight = tables[0, group : group + 1, :] * old
            straight = straight + tables[2, group : group + 1, :] * entry
            cross = tables[1, group : group + 1, :] * old
            cross = cross + tables[3, group : group + 1, :] * entry
            new = straight + pltpu.roll(cross, states, 1)
            new_carried[pl.ds(group, count_rows, stride=groups), :] = new
            high = new.astype(jnp.bfloat16)
            joined[block, :count_rows, columns] = high
            joined[block, count_rows:, columns] = (new - high.astype(jnp.float32)).astype(
                jnp.bfloat16
            )
        both = dot_transposed(joined[block], spread_out[block])
        read = both[:count_rows] + both[count_rows:]
        read = read + skip[lanes].reshape(1, LANES) * drive[:, lanes].astype(jnp.float32)
        activated[:, lanes] = gelu(read).astype(jnp.bfloat16)

    def remote(source, target, send, recv, place):
        return pltpu.make_async_remote_copy(
            src_ref=source,
            dst_ref=target,
            send_sem=send,
            recv_sem=recv,
            device_id=place,
            device_id_type=MESH,
        )

    def exchange(part):
        return remote(
            partial.at[part], partial_in.at[part], partial_send, partial_recv.at[part], (ep, other)
        )

    for part in range(OUT_PARTS):
        span = slice(part * out_span, (part + 1) * out_span)
        loads["w_out", part].wait()
        partial[part] = dot_wide(activated[...], mix[:, span]).astype(jnp.bfloat16)
        if part == 0:
            pl.semaphore_wait(barrier, EXPERTS + group_size - 1)
        exchange(part).start()
    weight_copies(down_hbm, down, weight_sem.at[1])

    loads["ids"].wait()
    loads["logit"].wait()
    loads["expert_gain"].wait()
    pack, weighed = routing(ids[...], logit[...])
    pack = pack.astype(jnp.bfloat16)
    weighed = weighed.T
    weight_high = weighed.astype(jnp.bfloat16)
    weight_low = (weighed - weight_high.astype(jnp.float32)).astype(jnp.bfloat16)

    for part in range(OUT_PARTS):
        span = slice(part * out_span, (part + 1) * out_span)
        exchange(part).wait_recv()
        summed = partial[part].astype(jnp.float32) + partial_in[part].astype(jnp.float32)
        mixed_buf[:, span] = (tokens[:, span].astype(jnp.float32) + summed).astype(jnp.bfloat16)
    normed_buf[...] = normalize(mixed_buf[...], expert_gain[...])

    def direct(index, step):
        place = at_expert(step)
        return remote(
            packed[index].at[place],
            rows_buf[index].at[core, lane, expert],
            direct_send.at[index],
            direct_recv.at[index, step],
            (place * group_size + lane, core),
        )

    def to_peer(index, step, shift):
        block = rows_buf[index].at[core, lane, at_expert(step)]
        place = (expert * group_size + at_lane(shift), core)
        return remote(block, block, peer_send.at[index], peer_recv.at[index, shift], place)

    def from_peer(index, shift):
        block = rows_buf[index].at[core, at_lane(-shift)]
        place = (expert * group_size + at_lane(shift), core)
        return remote(block, block, peer_send.at[index], peer_recv.at[index, shift], place)

    def across(index, shift):
        block = rows_buf[index].at[core, at_lane(-shift)]
        return remote(block, block, core_send.at[index], core_recv.at[index], (ep, other))

    def from_core(index):
        block = rows_buf[index].at[other]
        return remote(block, block, core_send.at[index], core_recv.at[index], (ep, other))

    for index, (begin, size) in enumerate(chunks):
        columns = pl.ds(pl.multiple_of(core * half + begin, LANES), size)
        chosen = dot_wide(pack, normed_buf[:, columns]).astype(jnp.bfloat16)
        packed[index][...] = chosen.reshape(EXPERTS, CAP, size)
        for step in SEND_ORDER:
            direct(index, step).start()
        rows_buf[index][core, lane, expert] = packed[index][expert]

    def relay(index):
        for step in WAIT_ORDER:
            if step:
                direct(index, step).wait_recv()
            for shift in range(1, group_size):
                to_peer(index, step, shift).start()
        across(index, 0).start()

    def cross(index):
        for shift in range(1, group_size):
            from_peer(index, shift).wait_recv()
            across(index, shift).start()

    height = hidden_units // UNIT_PARTS

    def accumulate(index, side, number, stage):
        begin, size = chunks[index]
        units = slice(number * height, (number + 1) * height)
        columns = pl.ds(pl.multiple_of(side * half + begin, LANES), size)
        arrived = rows_buf[index][side].reshape(total_rows, size)
        gated = dot_transposed(gate[units, columns], arrived)
        upward = dot_transposed(up[units, columns], arrived)
        if stage:
            gated = gate_sum[units, :] + gated
            upward = up_sum[units, :] + upward
        if stage < 2 * len(chunks) - 1:
            gate_sum[units, :] = gated
            up_sum[units, :] = upward
        else:
            hidden_t[units, :] = (jax.nn.silu(gated) * upward).astype(jnp.bfloat16)

    def transpose(begin, end):
        for start in range(begin, end, LANES):
            units = slice(start, min(start + LANES, end))
            hidden[:, units] = hidden_t[units, :].T

    relay(0)
    for index in range(len(chunks)):
        if index + 1 < len(chunks):
            relay(index + 1)
        if index == 0:
            cross(0)
            pltpu.make_async_copy(gate_up, gate_up, weight_sem.at[0]).wait()
        for number in range(UNIT_PARTS):
            accumulate(index, core, number, 2 * index)
        from_core(index).wait_recv()
        for number in range(UNIT_PARTS):
            accumulate(index, other, number, 2 * index + 1)
            if number == 0 and index + 1 < len(chunks):
                cross(index + 1)
    transpose(0, hidden_units)
    pltpu.make_async_copy(down, down, weight_sem.at[1]).wait()

    def produce(owner, index):
        begin, size = pieces[index]
        columns = pl.ds(pl.multiple_of(owner * half + begin, LANES), size)
        return jnp.dot(hidden[...], down[:, columns], preferred_element_type=jnp.float32)

    def swap(index):
        return remote(
            swap_out[index], swap_in[index], swap_send.at[index], swap_recv.at[index], (ep, other)
        )

    def sum_to_peer(index, shift):
        place = at_lane(shift)
        return remote(
            peer_out.at[index, place],
            peer_in.at[index, shift - 1],
            sum_send,
            sum_recv.at[index],
            (expert * group_size + place, core),
        )

    def from_peers(index):
        block = peer_in.at[index]
        return remote(block, block, sum_send, sum_recv.at[index], (ep, other))

    def give_back(index, step):
        place = at_expert(step)
        return remote(
            back_out.at[index, place],
            returned.at[index, expert],
            back_send,
            back_recv.at[index],
            (place * group_size + lane, core),
        )

    def given_back(index):
        block = returned.at[index, : EXPERTS - 1]
        return remote(block, block, back_send, back_recv.at[index], (ep, other))

    def start_swap(index):
        swap_out[index][...] = produce(other, index).astype(jnp.bfloat16)
        swap(index).start()

    start_swap(0)
    for index, (begin, size) in enumerate(pieces):
        if index + 1 < len(pieces):
            start_swap(index + 1)
        value = produce(core, index)
        swap(index).wait_recv()
        value = value + swap_in[index][...].astype(jnp.float32)
        for inner in range(0, size, STRIP):
            strip = (begin + inner) // STRIP
            shape = (group_size, EXPERTS, CAP, STRIP)
            columns = value[:, inner : inner + STRIP].reshape(shape)
            own_sum[strip] = columns
            peer_out[strip] = columns.astype(jnp.bfloat16)
            for shift in range(1, group_size):
                sum_to_peer(strip, shift).start()
    for index in range(strips):
        value = own_sum[index, lane]
        if group_size > 1:
            from_peers(index).wait_recv()
        for shift in range(1, group_size):
            value = value + peer_in[index, shift - 1].astype(jnp.float32)
        back_out[index] = value.astype(jnp.bfloat16)
        for step in BACK_ORDER:
            give_back(index, step).start()
        returned[index, expert] = back_out[index, expert]
    for index in range(strips):
        given_back(index).wait_recv()
        rows = returned[index].reshape(EXPERTS * CAP, STRIP)
        value = jnp.dot(weight_high, rows, preferred_element_type=jnp.float32)
        value = value + jnp.dot(weight_low, rows, preferred_element_type=jnp.float32)
        columns = pl.ds(pl.multiple_of(core * half + index * STRIP, LANES), STRIP)
        value = value + mixed_buf[:, columns].astype(jnp.float32)
        out[:, index * STRIP : (index + 1) * STRIP] = value.astype(out.dtype)

    def sent(block, sem):
        remote(block, block, sem, sem, (ep, other)).wait_send()

    sent(partial, partial_send)
    for index in range(len(chunks)):
        sent(packed[index].at[: EXPERTS - 1], direct_send.at[index])
        if group_size > 1:
            sent(rows_buf[index].at[core, : group_size - 1], peer_send.at[index])
        sent(rows_buf[index].at[core], core_send.at[index])
    for index in range(len(pieces)):
        sent(swap_out[index], swap_send.at[index])
    if group_size > 1:
        sent(peer_out.at[:, : group_size - 1], sum_send)
    sent(back_out.at[:, : EXPERTS - 1], back_send)


def per_device(
    tokens,
    carried,
    decay_rate,
    frequency,
    log_step,
    in_map,
    out_map,
    skip_gain,
    norm_gain,
    w_in,
    w_out,
    expert_gain,
    route_ids,
    route_logit,
    w_gate,
    w_up,
    w_down,
):
    count_rows, model_width = tokens.shape
    groups, states = decay_rate.shape
    width = skip_gain.shape[0]
    per_block = LANES * groups // width
    blocks = groups // per_block
    sources = lax.axis_size("ep")
    group_size = sources // EXPERTS
    half = model_width // 2
    pieces = parts_of(half, PIECE_SHARES)
    strips = half // STRIP
    chunks = parts_of(half, CHUNK_SHARES)
    hidden_units = w_down.shape[0]
    total_rows = sources * CAP
    peers = max(group_size - 1, 1)
    dma = pltpu.SemaphoreType.DMA
    narrow = jnp.bfloat16
    wide = jnp.float32
    vmem = pl.BlockSpec(memory_space=pltpu.VMEM)
    far = pl.BlockSpec(memory_space=pltpu.HBM)
    operands = (
        tokens,
        carried.reshape(count_rows * groups, 2 * states),
        decay_rate,
        frequency,
        log_step.reshape(1, groups),
        in_map.transpose(0, 2, 1).reshape(width, 2 * states),
        out_map.reshape(width, 2 * states),
        skip_gain,
        norm_gain.reshape(1, model_width),
        w_in,
        w_out,
        expert_gain.reshape(1, model_width),
        route_ids.T,
        route_logit.T,
        w_gate.T,
        w_up.T,
        w_down,
    )
    staged = operands[:9] + operands[11:14]

    def each(parts, shape, dtype=narrow):
        return tuple(pltpu.VMEM((*shape, size), dtype) for _, size in parts)

    new_tokens, new_carried = pl.pallas_call(
        functools.partial(layer_kernel, group_size),
        out_shape=(
            jax.ShapeDtypeStruct((count_rows, half), narrow),
            jax.ShapeDtypeStruct((count_rows * groups, 2 * states), wide),
        ),
        in_specs=[far] * len(operands),
        out_specs=(vmem, vmem),
        scratch_shapes=[pltpu.VMEM(value.shape, value.dtype) for value in staged]
        + [
            pltpu.VMEM((2, hidden_units, model_width), narrow),
            pltpu.VMEM((max(2 * width, hidden_units), model_width), narrow),
            pltpu.VMEM((4, groups, 2 * states), wide),
            pltpu.VMEM((blocks, LANES, per_block * LANES), narrow),
            pltpu.VMEM((blocks, LANES, per_block * LANES), narrow),
            pltpu.VMEM((blocks, 2 * count_rows, per_block * LANES), narrow),
            pltpu.VMEM((count_rows, width), narrow),
            pltpu.VMEM((OUT_PARTS, count_rows, model_width // OUT_PARTS), narrow),
            pltpu.VMEM((OUT_PARTS, count_rows, model_width // OUT_PARTS), narrow),
            pltpu.VMEM((count_rows, model_width), narrow),
            pltpu.VMEM((count_rows, model_width), narrow),
            each(chunks, (EXPERTS, CAP)),
            each(chunks, (2, group_size, EXPERTS, CAP)),
            pltpu.VMEM((hidden_units, total_rows), wide),
            pltpu.VMEM((hidden_units, total_rows), wide),
            pltpu.VMEM((hidden_units, total_rows), narrow),
            pltpu.VMEM((total_rows, hidden_units), narrow),
            each(pieces, (total_rows,)),
            each(pieces, (total_rows,)),
            pltpu.VMEM((strips, group_size, EXPERTS, CAP, STRIP), wide),
            pltpu.VMEM((strips, group_size, EXPERTS, CAP, STRIP), narrow),
            pltpu.VMEM((strips, peers, EXPERTS, CAP, STRIP), narrow),
            pltpu.VMEM((strips, EXPERTS, CAP, STRIP), narrow),
            pltpu.VMEM((strips, EXPERTS, CAP, STRIP), narrow),
            dma((len(staged) + model_width // width + OUT_PARTS,)),
            dma((2,)),
            dma,
            dma((OUT_PARTS,)),
            dma((len(chunks),)),
            dma((len(chunks), EXPERTS)),
            dma((len(chunks),)),
            dma((len(chunks), group_size)),
            dma((len(chunks),)),
            dma((len(chunks),)),
            dma((len(pieces),)),
            dma((len(pieces),)),
            dma,
            dma((strips,)),
            dma,
            dma((strips,)),
        ],
        compiler_params=pltpu.CompilerParams(
            collective_id=0, has_side_effects=True, vmem_limit_bytes=50 * 1024 * 1024
        ),
    )(*[pltpu.with_memory_space_constraint(value, pltpu.HBM) for value in operands])
    return (new_tokens, new_carried.reshape(count_rows, groups, 2 * states))


def solution(mesh):
    return jax.shard_map(
        per_device,
        mesh=mesh,
        in_specs=(
            P("ep", None),
            P("ep", "tp", None),
            P("tp", None),
            P("tp", None),
            P("tp"),
            P("tp", None, None),
            P("tp", None, None),
            P("tp"),
            P(),
            P(None, "tp"),
            P("tp", None),
            P(),
            P("ep", None),
            P("ep", None),
            P(None, ("ep", "tp")),
            P(None, ("ep", "tp")),
            P(("ep", "tp"), None),
        ),
        out_specs=(P("ep", "tp"), P("ep", "tp", None)),
        check_vma=False,
    )
```

```python
import functools

import jax
import jax.numpy as jnp
from jax import lax
from jax.experimental import pallas as pl
from jax.experimental.pallas import tpu as pltpu
from jax.sharding import PartitionSpec as P

EXPERTS = 8
TOP = 2
CAP = 16

MESH = pl.DeviceIdType.MESH
SEND_ORDER = (1, 3, 2, 5, 4, 7, 6)
WAIT_ORDER = (0, 1, 2, 3, 4, 5, 6, 7)
BACK_ORDER = (4, 6, 5, 7, 2, 3, 1)
CHUNK_SHARES = (3, 3)
PIECE_SHARES = (2, 2, 2)
STRIP = 256
UNIT_PARTS = 1
LANES = 128
LATE_PART = 1
OUT_PARTS = 2
WEIGHT_PARTS = 3


def parts_of(length, shares):
    unit = length // sum(shares)
    starts = [unit * sum(shares[:index]) for index in range(len(shares))]
    return [(start, unit * share) for start, share in zip(starts, shares)]


def normalize(rows, gain):
    wide = rows.astype(jnp.float32)
    scaled = wide * lax.rsqrt(jnp.mean(wide * wide, axis=-1, keepdims=True) + 1e-06)
    return (scaled * gain).astype(jnp.bfloat16)


def dot_wide(left, right):
    return jnp.dot(left, right, preferred_element_type=jnp.float32)


def dot_transposed(left, right):
    return lax.dot_general(
        left, right, (((1,), (1,)), ((), ())), preferred_element_type=jnp.float32
    )


def gelu(value):
    inner = 0.7978845608028654 * (value + 0.044715 * (value * value * value))
    return value * (0.5 * (1.0 + jnp.tanh(inner)))


def coefficients(log_step, decay_rate, frequency, tables):
    groups, half = decay_rate.shape
    row = lax.broadcasted_iota(jnp.int32, (groups, groups), 0)
    column = lax.broadcasted_iota(jnp.int32, (groups, groups), 1)
    spread = jnp.where(row == column, jnp.broadcast_to(log_step, (groups, groups)), 0.0)
    step_size = jnp.exp(jnp.sum(spread, axis=1, keepdims=True))
    magnitude = jnp.exp(-decay_rate * step_size)
    real_decay = magnitude * jnp.cos(frequency * step_size)
    imag_decay = magnitude * jnp.sin(frequency * step_size)
    denom = decay_rate * decay_rate + frequency * frequency
    real_less = real_decay - 1.0
    real_factor = (-real_less * decay_rate + imag_decay * frequency) / denom
    imag_factor = (-imag_decay * decay_rate - real_less * frequency) / denom
    tables[0] = jnp.concatenate([real_decay, real_decay], axis=1)
    tables[1] = jnp.concatenate([imag_decay, -imag_decay], axis=1)
    tables[2] = jnp.concatenate([real_factor, real_factor], axis=1)
    tables[3] = jnp.concatenate([imag_factor, -imag_factor], axis=1)


def routing(ids, logit):
    count_rows = ids.shape[1]
    expert = lax.broadcasted_iota(jnp.int32, (EXPERTS, count_rows), 0)
    first = (ids[0:1, :] == expert).astype(jnp.float32)
    second = (ids[1:2, :] == expert).astype(jnp.float32)
    named = first + second
    weight = first * jax.nn.sigmoid(logit[0:1, :] - logit[1:2, :])
    weight = weight + second * jax.nn.sigmoid(logit[1:2, :] - logit[0:1, :])
    row = lax.broadcasted_iota(jnp.int32, (count_rows, count_rows), 0)
    column = lax.broadcasted_iota(jnp.int32, (count_rows, count_rows), 1)
    earlier = dot_wide(named, (row < column).astype(jnp.float32))
    slots = (EXPERTS, CAP, count_rows)
    slot = lax.broadcasted_iota(jnp.int32, slots, 1).astype(jnp.float32)
    here = slot == jnp.broadcast_to(earlier[:, None, :], slots)
    pack = jnp.where(here, jnp.broadcast_to(named[:, None, :], slots), 0.0)
    weighed = jnp.where(here, jnp.broadcast_to(weight[:, None, :], slots), 0.0)
    total = EXPERTS * CAP
    return pack.reshape(total, count_rows), weighed.reshape(total, count_rows)


def layer_kernel(
    group_size,
    tokens_hbm,
    carried_hbm,
    decay_hbm,
    frequency_hbm,
    log_step_hbm,
    in_map_hbm,
    out_map_hbm,
    skip_hbm,
    norm_gain_hbm,
    w_in_hbm,
    w_out_hbm,
    expert_gain_hbm,
    ids_hbm,
    logit_hbm,
    gate_hbm,
    up_hbm,
    down_hbm,
    out,
    new_carried,
    tokens,
    carried,
    decay_rate,
    frequency,
    log_step,
    in_map,
    out_map,
    skip,
    norm_gain,
    expert_gain,
    ids,
    logit,
    gate_up,
    dense,
    tables,
    spread_in,
    spread_out,
    joined,
    activated,
    partial,
    partial_in,
    mixed_buf,
    normed_buf,
    packed,
    rows_buf,
    gate_sum,
    up_sum,
    hidden_t,
    hidden,
    swap_out,
    swap_in,
    own_sum,
    peer_out,
    peer_in,
    back_out,
    returned,
    load_sem,
    weight_sem,
    partial_send,
    partial_recv,
    direct_send,
    direct_recv,
    peer_send,
    peer_recv,
    core_send,
    core_recv,
    swap_send,
    swap_recv,
    sum_send,
    sum_recv,
    back_send,
    back_recv,
):
    ep = lax.axis_index("ep")
    core = lax.axis_index("tp")
    expert = ep // group_size
    lane = ep % group_size
    other = 1 - core
    count_rows, model_width = tokens.shape
    groups, states = decay_rate.shape
    width = skip.shape[0]
    channels = width // groups
    per_block = LANES // channels
    blocks = groups // per_block
    half = model_width // 2
    hidden_units = gate_hbm.shape[0]
    total_rows = group_size * EXPERTS * CAP
    in_parts = model_width // width
    gate, up = gate_up.at[0], gate_up.at[1]
    mix = dense.at[width : 2 * width]
    down = dense.at[:hidden_units]
    pieces = parts_of(half, PIECE_SHARES)
    strips = half // STRIP
    chunks = parts_of(half, CHUNK_SHARES)

    def at_expert(step):
        place, bit = 0, 1
        while bit < EXPERTS:
            place = place + bit * lax.rem(expert // bit + step // bit, 2)
            bit *= 2
        return place

    def at_lane(step):
        return lax.rem(lane + step + group_size, group_size)

    loads = {}

    def load(name, source, target):
        loads[name] = pltpu.make_async_copy(source, target, load_sem.at[len(loads)])
        loads[name].start()

    load("tokens", tokens_hbm, tokens)
    load("norm_gain", norm_gain_hbm, norm_gain)
    for part in range(in_parts):
        span = pl.ds(part * width, width)
        load(("w_in", part), w_in_hbm.at[span], dense.at[:width, span])
    load("log_step", log_step_hbm, log_step)
    load("decay", decay_hbm, decay_rate)
    load("frequency", frequency_hbm, frequency)
    load("in_map", in_map_hbm, in_map)
    load("out_map", out_map_hbm, out_map)
    load("carried", carried_hbm, carried)
    load("skip", skip_hbm, skip)
    load("ids", ids_hbm, ids)
    load("logit", logit_hbm, logit)
    load("expert_gain", expert_gain_hbm, expert_gain)
    out_span = model_width // OUT_PARTS

    barrier = pltpu.get_barrier_semaphore()
    pl.semaphore_signal(barrier, inc=1, device_id=(ep, other), device_id_type=MESH)
    for step in range(1, EXPERTS):
        target = at_expert(step) * group_size + lane
        pl.semaphore_signal(barrier, inc=1, device_id=(target, core), device_id_type=MESH)
    for step in range(1, group_size):
        target = expert * group_size + at_lane(step)
        pl.semaphore_signal(barrier, inc=1, device_id=(target, core), device_id_type=MESH)

    weight_span = hidden_units // WEIGHT_PARTS

    def weight_copies(source, target, sem):
        for part in range(WEIGHT_PARTS):
            span = pl.ds(part * weight_span, weight_span)
            pltpu.make_async_copy(source.at[span], target.at[span], sem).start()

    spread_in[...] = jnp.zeros_like(spread_in)
    spread_out[...] = jnp.zeros_like(spread_out)
    loads["tokens"].wait()
    loads["norm_gain"].wait()
    normed_buf[...] = normalize(tokens[...], norm_gain[...])
    for name in ("log_step", "decay", "frequency"):
        loads[name].wait()
    coefficients(log_step[...], decay_rate[...], frequency[...], tables)
    loads["in_map"].wait()
    loads["out_map"].wait()
    sign = jnp.where(lax.broadcasted_iota(jnp.int32, (1, LANES), 1) < states, 1.0, -1.0)
    for group in range(groups):
        block, place = divmod(group, per_block)
        rows = slice(place * channels, (place + 1) * channels)
        columns = slice(place * LANES, (place + 1) * LANES)
        tile = slice(group * channels, (group + 1) * channels)
        spread_in[block, rows, columns] = in_map[tile, :]
        spread_out[block, rows, columns] = (out_map[tile, :].astype(jnp.float32) * sign).astype(
            jnp.bfloat16
        )
    total = None
    for part in range(in_parts):
        loads["w_in", part].wait()
        if part == LATE_PART:
            for late in range(OUT_PARTS):
                span = pl.ds(late * out_span, out_span)
                load(("w_out", late), w_out_hbm.at[:, span], mix.at[:, span])
        span = slice(part * width, (part + 1) * width)
        term = dot_wide(normed_buf[:, span], dense[:width, span])
        total = term if total is None else total + term
    drive = total.astype(jnp.bfloat16)
    loads["carried"].wait()
    loads["skip"].wait()
    weight_copies(gate_hbm, gate, weight_sem.at[0])
    weight_copies(up_hbm, up, weight_sem.at[0])
    for block in range(blocks):
        lanes = slice(block * LANES, (block + 1) * LANES)
        projected = dot_wide(drive[:, lanes], spread_in[block])
        for place in range(per_block):
            group = block * per_block + place
            columns = slice(place * LANES, (place + 1) * LANES)
            entry = projected[:, columns]
            old = carried[pl.ds(group, count_rows, stride=groups), :]
            straight = tables[0, group : group + 1, :] * old
            straight = straight + tables[2, group : group + 1, :] * entry
            cross = tables[1, group : group + 1, :] * old
            cross = cross + tables[3, group : group + 1, :] * entry
            new = straight + pltpu.roll(cross, states, 1)
            new_carried[pl.ds(group, count_rows, stride=groups), :] = new
            high = new.astype(jnp.bfloat16)
            joined[block, :count_rows, columns] = high
            joined[block, count_rows:, columns] = (new - high.astype(jnp.float32)).astype(
                jnp.bfloat16
            )
        both = dot_transposed(joined[block], spread_out[block])
        read = both[:count_rows] + both[count_rows:]
        read = read + skip[lanes].reshape(1, LANES) * drive[:, lanes].astype(jnp.float32)
        activated[:, lanes] = gelu(read).astype(jnp.bfloat16)

    def remote(source, target, send, recv, place):
        return pltpu.make_async_remote_copy(
            src_ref=source,
            dst_ref=target,
            send_sem=send,
            recv_sem=recv,
            device_id=place,
            device_id_type=MESH,
        )

    def exchange(part):
        return remote(
            partial.at[part], partial_in.at[part], partial_send, partial_recv.at[part], (ep, other)
        )

    for part in range(OUT_PARTS):
        span = slice(part * out_span, (part + 1) * out_span)
        loads["w_out", part].wait()
        partial[part] = dot_wide(activated[...], mix[:, span]).astype(jnp.bfloat16)
        if part == 0:
            pl.semaphore_wait(barrier, EXPERTS + group_size - 1)
        exchange(part).start()
    weight_copies(down_hbm, down, weight_sem.at[1])

    loads["ids"].wait()
    loads["logit"].wait()
    loads["expert_gain"].wait()
    pack, weighed = routing(ids[...], logit[...])
    pack = pack.astype(jnp.bfloat16)
    weighed = weighed.T
    weight_high = weighed.astype(jnp.bfloat16)
    weight_low = (weighed - weight_high.astype(jnp.float32)).astype(jnp.bfloat16)

    for part in range(OUT_PARTS):
        span = slice(part * out_span, (part + 1) * out_span)
        exchange(part).wait_recv()
        summed = partial[part].astype(jnp.float32) + partial_in[part].astype(jnp.float32)
        mixed_buf[:, span] = (tokens[:, span].astype(jnp.float32) + summed).astype(jnp.bfloat16)
    normed_buf[...] = normalize(mixed_buf[...], expert_gain[...])

    def direct(index, step):
        place = at_expert(step)
        return remote(
            packed[index].at[place],
            rows_buf[index].at[core, lane, expert],
            direct_send.at[index],
            direct_recv.at[index, step],
            (place * group_size + lane, core),
        )

    def to_peer(index, step, shift):
        block = rows_buf[index].at[core, lane, at_expert(step)]
        place = (expert * group_size + at_lane(shift), core)
        return remote(block, block, peer_send.at[index], peer_recv.at[index, shift], place)

    def from_peer(index, shift):
        block = rows_buf[index].at[core, at_lane(-shift)]
        place = (expert * group_size + at_lane(shift), core)
        return remote(block, block, peer_send.at[index], peer_recv.at[index, shift], place)

    def across(index, shift):
        block = rows_buf[index].at[core, at_lane(-shift)]
        return remote(block, block, core_send.at[index], core_recv.at[index], (ep, other))

    def from_core(index):
        block = rows_buf[index].at[other]
        return remote(block, block, core_send.at[index], core_recv.at[index], (ep, other))

    for index, (begin, size) in enumerate(chunks):
        columns = pl.ds(pl.multiple_of(core * half + begin, LANES), size)
        chosen = dot_wide(pack, normed_buf[:, columns]).astype(jnp.bfloat16)
        packed[index][...] = chosen.reshape(EXPERTS, CAP, size)
        for step in SEND_ORDER:
            direct(index, step).start()
        rows_buf[index][core, lane, expert] = packed[index][expert]

    def relay(index):
        for step in WAIT_ORDER:
            if step:
                direct(index, step).wait_recv()
            for shift in range(1, group_size):
                to_peer(index, step, shift).start()
        across(index, 0).start()

    def cross(index):
        for shift in range(1, group_size):
            from_peer(index, shift).wait_recv()
            across(index, shift).start()

    height = hidden_units // UNIT_PARTS

    def accumulate(index, side, number, stage):
        begin, size = chunks[index]
        units = slice(number * height, (number + 1) * height)
        columns = pl.ds(pl.multiple_of(side * half + begin, LANES), size)
        arrived = rows_buf[index][side].reshape(total_rows, size)
        gated = dot_transposed(gate[units, columns], arrived)
        upward = dot_transposed(up[units, columns], arrived)
        if stage:
            gated = gate_sum[units, :] + gated
            upward = up_sum[units, :] + upward
        if stage < 2 * len(chunks) - 1:
            gate_sum[units, :] = gated
            up_sum[units, :] = upward
        else:
            hidden_t[units, :] = (jax.nn.silu(gated) * upward).astype(jnp.bfloat16)

    def transpose(begin, end):
        for start in range(begin, end, LANES):
            units = slice(start, min(start + LANES, end))
            hidden[:, units] = hidden_t[units, :].T

    relay(0)
    for index in range(len(chunks)):
        if index + 1 < len(chunks):
            relay(index + 1)
        if index == 0:
            cross(0)
            pltpu.make_async_copy(gate_up, gate_up, weight_sem.at[0]).wait()
        for number in range(UNIT_PARTS):
            accumulate(index, core, number, 2 * index)
        from_core(index).wait_recv()
        for number in range(UNIT_PARTS):
            accumulate(index, other, number, 2 * index + 1)
            if number == 0 and index + 1 < len(chunks):
                cross(index + 1)
    transpose(0, hidden_units)
    pltpu.make_async_copy(down, down, weight_sem.at[1]).wait()

    def produce(owner, index):
        begin, size = pieces[index]
        columns = pl.ds(pl.multiple_of(owner * half + begin, LANES), size)
        return jnp.dot(hidden[...], down[:, columns], preferred_element_type=jnp.float32)

    def swap(index):
        return remote(
            swap_out[index], swap_in[index], swap_send.at[index], swap_recv.at[index], (ep, other)
        )

    def sum_to_peer(index, shift):
        place = at_lane(shift)
        return remote(
            peer_out.at[index, place],
            peer_in.at[index, shift - 1],
            sum_send,
            sum_recv.at[index],
            (expert * group_size + place, core),
        )

    def from_peers(index):
        block = peer_in.at[index]
        return remote(block, block, sum_send, sum_recv.at[index], (ep, other))

    def give_back(index, step):
        place = at_expert(step)
        return remote(
            back_out.at[index, place],
            returned.at[index, expert],
            back_send,
            back_recv.at[index],
            (place * group_size + lane, core),
        )

    def given_back(index):
        block = returned.at[index, : EXPERTS - 1]
        return remote(block, block, back_send, back_recv.at[index], (ep, other))

    def start_swap(index):
        swap_out[index][...] = produce(other, index).astype(jnp.bfloat16)
        swap(index).start()

    start_swap(0)
    for index, (begin, size) in enumerate(pieces):
        if index + 1 < len(pieces):
            start_swap(index + 1)
        value = produce(core, index)
        swap(index).wait_recv()
        value = value + swap_in[index][...].astype(jnp.float32)
        for inner in range(0, size, STRIP):
            strip = (begin + inner) // STRIP
            shape = (group_size, EXPERTS, CAP, STRIP)
            columns = value[:, inner : inner + STRIP].reshape(shape)
            own_sum[strip] = columns
            peer_out[strip] = columns.astype(jnp.bfloat16)
            for shift in range(1, group_size):
                sum_to_peer(strip, shift).start()
    for index in range(strips):
        value = own_sum[index, lane]
        if group_size > 1:
            from_peers(index).wait_recv()
        for shift in range(1, group_size):
            value = value + peer_in[index, shift - 1].astype(jnp.float32)
        back_out[index] = value.astype(jnp.bfloat16)
        for step in BACK_ORDER:
            give_back(index, step).start()
        returned[index, expert] = back_out[index, expert]
    for index in range(strips):
        given_back(index).wait_recv()
        rows = returned[index].reshape(EXPERTS * CAP, STRIP)
        value = jnp.dot(weight_high, rows, preferred_element_type=jnp.float32)
        value = value + jnp.dot(weight_low, rows, preferred_element_type=jnp.float32)
        columns = pl.ds(pl.multiple_of(core * half + index * STRIP, LANES), STRIP)
        value = value + mixed_buf[:, columns].astype(jnp.float32)
        out[:, index * STRIP : (index + 1) * STRIP] = value.astype(out.dtype)

    def sent(block, sem):
        remote(block, block, sem, sem, (ep, other)).wait_send()

    sent(partial, partial_send)
    for index in range(len(chunks)):
        sent(packed[index].at[: EXPERTS - 1], direct_send.at[index])
        if group_size > 1:
            sent(rows_buf[index].at[core, : group_size - 1], peer_send.at[index])
        sent(rows_buf[index].at[core], core_send.at[index])
    for index in range(len(pieces)):
        sent(swap_out[index], swap_send.at[index])
    if group_size > 1:
        sent(peer_out.at[:, : group_size - 1], sum_send)
    sent(back_out.at[:, : EXPERTS - 1], back_send)


def per_device(
    tokens,
    carried,
    decay_rate,
    frequency,
    log_step,
    in_map,
    out_map,
    skip_gain,
    norm_gain,
    w_in,
    w_out,
    expert_gain,
    route_ids,
    route_logit,
    w_gate,
    w_up,
    w_down,
):
    count_rows, model_width = tokens.shape
    groups, states = decay_rate.shape
    width = skip_gain.shape[0]
    per_block = LANES * groups // width
    blocks = groups // per_block
    sources = lax.axis_size("ep")
    group_size = sources // EXPERTS
    half = model_width // 2
    pieces = parts_of(half, PIECE_SHARES)
    strips = half // STRIP
    chunks = parts_of(half, CHUNK_SHARES)
    hidden_units = w_down.shape[0]
    total_rows = sources * CAP
    peers = max(group_size - 1, 1)
    dma = pltpu.SemaphoreType.DMA
    narrow = jnp.bfloat16
    wide = jnp.float32
    vmem = pl.BlockSpec(memory_space=pltpu.VMEM)
    far = pl.BlockSpec(memory_space=pltpu.HBM)
    operands = (
        tokens,
        carried.reshape(count_rows * groups, 2 * states),
        decay_rate,
        frequency,
        log_step.reshape(1, groups),
        in_map.transpose(0, 2, 1).reshape(width, 2 * states),
        out_map.reshape(width, 2 * states),
        skip_gain,
        norm_gain.reshape(1, model_width),
        w_in,
        w_out,
        expert_gain.reshape(1, model_width),
        route_ids.T,
        route_logit.T,
        w_gate.T,
        w_up.T,
        w_down,
    )
    staged = operands[:9] + operands[11:14]

    def each(parts, shape, dtype=narrow):
        return tuple(pltpu.VMEM((*shape, size), dtype) for _, size in parts)

    new_tokens, new_carried = pl.pallas_call(
        functools.partial(layer_kernel, group_size),
        out_shape=(
            jax.ShapeDtypeStruct((count_rows, half), narrow),
            jax.ShapeDtypeStruct((count_rows * groups, 2 * states), wide),
        ),
        in_specs=[far] * len(operands),
        out_specs=(vmem, vmem),
        scratch_shapes=[pltpu.VMEM(value.shape, value.dtype) for value in staged]
        + [
            pltpu.VMEM((2, hidden_units, model_width), narrow),
            pltpu.VMEM((max(2 * width, hidden_units), model_width), narrow),
            pltpu.VMEM((4, groups, 2 * states), wide),
            pltpu.VMEM((blocks, LANES, per_block * LANES), narrow),
            pltpu.VMEM((blocks, LANES, per_block * LANES), narrow),
            pltpu.VMEM((blocks, 2 * count_rows, per_block * LANES), narrow),
            pltpu.VMEM((count_rows, width), narrow),
            pltpu.VMEM((OUT_PARTS, count_rows, model_width // OUT_PARTS), narrow),
            pltpu.VMEM((OUT_PARTS, count_rows, model_width // OUT_PARTS), narrow),
            pltpu.VMEM((count_rows, model_width), narrow),
            pltpu.VMEM((count_rows, model_width), narrow),
            each(chunks, (EXPERTS, CAP)),
            each(chunks, (2, group_size, EXPERTS, CAP)),
            pltpu.VMEM((hidden_units, total_rows), wide),
            pltpu.VMEM((hidden_units, total_rows), wide),
            pltpu.VMEM((hidden_units, total_rows), narrow),
            pltpu.VMEM((total_rows, hidden_units), narrow),
            each(pieces, (total_rows,)),
            each(pieces, (total_rows,)),
            pltpu.VMEM((strips, group_size, EXPERTS, CAP, STRIP), wide),
            pltpu.VMEM((strips, group_size, EXPERTS, CAP, STRIP), narrow),
            pltpu.VMEM((strips, peers, EXPERTS, CAP, STRIP), narrow),
            pltpu.VMEM((strips, EXPERTS, CAP, STRIP), narrow),
            pltpu.VMEM((strips, EXPERTS, CAP, STRIP), narrow),
            dma((len(staged) + model_width // width + OUT_PARTS,)),
            dma((2,)),
            dma,
            dma((OUT_PARTS,)),
            dma((len(chunks),)),
            dma((len(chunks), EXPERTS)),
            dma((len(chunks),)),
            dma((len(chunks), group_size)),
            dma((len(chunks),)),
            dma((len(chunks),)),
            dma((len(pieces),)),
            dma((len(pieces),)),
            dma,
            dma((strips,)),
            dma,
            dma((strips,)),
        ],
        compiler_params=pltpu.CompilerParams(
            collective_id=0, has_side_effects=True, vmem_limit_bytes=50 * 1024 * 1024
        ),
    )(*[pltpu.with_memory_space_constraint(value, pltpu.HBM) for value in operands])
    return (new_tokens, new_carried.reshape(count_rows, groups, 2 * states))


def solution(mesh):
    return jax.shard_map(
        per_device,
        mesh=mesh,
        in_specs=(
            P("ep", None),
            P("ep", "tp", None),
            P("tp", None),
            P("tp", None),
            P("tp"),
            P("tp", None, None),
            P("tp", None, None),
            P("tp"),
            P(),
            P(None, "tp"),
            P("tp", None),
            P(),
            P("ep", None),
            P("ep", None),
            P(None, ("ep", "tp")),
            P(None, ("ep", "tp")),
            P(("ep", "tp"), None),
        ),
        out_specs=(P("ep", "tp"), P("ep", "tp", None)),
        check_vma=False,
    )
```
